32 devices in a mesh: kv: 8 (over z, y), tp: 4 (over x, core).
Axes of the slice: x: 2, y: 2, z: 4, core: 2. Of those that a mesh axis runs over, the one named last changes fastest.
Arguments:
- piece_tokens: bfloat16 [32, 2048], P('kv'), may hold values from -6 to 6
- decode_tokens: bfloat16 [8, 2048], P('kv'), may hold values from -6 to 6
- prompt_fill: int32 [1], replicated, may hold values from 1024 to 2016
- decode_fill: int32 [8], P('kv'), may hold values from 1 to 767, 3072 in all
- prompt_cache: bfloat16 [2048, 544], P('kv'), may hold values from -600 to 600
- decode_cache: bfloat16 [8, 768, 544], P('kv'), may hold values from -600 to 600
- input_gain: float32 [2048], replicated, may hold values from 0.1 to 1.9
- query_gain: float32 [768], replicated, may hold values from 0.1 to 1.9
- latent_gain: float32 [512], replicated, may hold values from 0.1 to 1.9
- query_down: bfloat16 [2048, 768], P(None, 'tp'), may hold values from -0.125 to 0.125
- latent_down: bfloat16 [2048, 512], P(None, 'tp'), may hold values from -0.125 to 0.125
- rope_down: bfloat16 [2048, 32], replicated, may hold values from -0.125 to 0.125
- query_up: bfloat16 [768, 1024], P(None, 'tp'), may hold values from -0.21875 to 0.21875
- qrope_up: bfloat16 [768, 512], P(None, 'tp'), may hold values from -0.21875 to 0.21875
- key_up: bfloat16 [16, 64, 512], P('tp'), may hold values from -0.25 to 0.25
- value_up: bfloat16 [16, 512, 64], P('tp'), may hold values from -4 to 4
- out_proj: bfloat16 [1024, 2048], P('tp'), may hold values from -4 to 4
Outputs:
- piece_out: bfloat16 [32, 2048], P('kv')
- decode_out: bfloat16 [8, 2048], P('kv')
- piece_rows: bfloat16 [32, 544], P('kv')
- decode_rows: bfloat16 [8, 544], P('kv')
The draws below stay inside these ranges and needn't reach their ends.
Inputs may be any that keep to these rules, and one draw needn't show every extreme that they name: `prompt_fill`: the piece takes the 32 positions that follow the cache's filled positions. `decode_fill`: a decoding sequence's new token takes the position that follows its filled ones.
All inputs are finite; a program needn't handle non-finite values. No bound on the sum of `decode_fill` on one device may be relied on, other than what follows from the above.
Results may differ from the reference program's by a relative error of at most 0.035.
Values may be sent and summed in bfloat16 or wider, within the bound.
A program may use at most 64 MiB of HBM per device.

```python
import math
import jax
import jax.numpy as jnp
import numpy as np
from jax import lax

D = 2048
H = 16
QL = 768
KL = 512
NOPE = 64
ROPE = 32
VD = 64
CACHE_DEV = 256
DEC_LEN = 768
PIECE = 32
CACHE = 2048
DEC = 8
N_KV = 8
N_TP = 4


def draw_prompt_cache(key, part):
    values = jnp.clip(jax.random.normal(key, (CACHE, KL + ROPE), jnp.float32), -5.0, 5.0)
    return values.astype(jnp.bfloat16)


def draw_decode_cache(key, part):
    values = jnp.clip(jax.random.normal(key, (DEC, DEC_LEN, KL + ROPE), jnp.float32), -5.0, 5.0)
    return values.astype(jnp.bfloat16)


def block_levels(key, dims, pieces, least, largest):
    def one(position, shards_of):
        draws = jax.random.uniform(jax.random.fold_in(jax.random.fold_in(key, 6), position), (shards_of,), jnp.float32, least / len(pieces), largest / len(pieces))
        return jnp.repeat(jnp.exp(draws), dims[position] // shards_of).reshape((-1,) + (1,) * (len(dims) - position - 1))

    gain = one(*pieces[0])
    for cut in pieces[1:]:
        gain = gain * one(*cut)
    return gain


def profile(amount, total, most, slope):
    weights = [(1 << 20) // math.isqrt(grade ** slope) + 1 for grade in range(2, amount + 1)]
    rest, holding = total - most - (amount - 1), [1] * (amount - 1)
    while rest > 0:
        candidates = [i for i in range(amount - 1) if holding[i] < most]
        whole, left = sum([weights[i] for i in candidates]), rest
        for i in candidates:
            extra = min(most - holding[i], max(1, left * weights[i] // whole), rest)
            holding[i] = holding[i] + extra
            rest = rest - extra
    return np.array([most] + holding)


def uneven(rng, amount, total, most, skew):
    if amount == 2:
        one = jax.random.randint(rng, (), max(1, total - most), min(most, total - 1) + 1)
        return jnp.stack([one, total - one])
    tallies = jnp.asarray(profile(amount, total, most, skew), jnp.int32)
    couples = (amount - 1) // 2
    donor, receiver = tallies[1:1 + 2 * couples:2], tallies[2:2 + 2 * couples:2]
    margin = jnp.minimum(donor - 1, most - receiver)
    moved = jax.random.randint(jax.random.fold_in(rng, 1), (couples,), 0, 1 << 20) % (margin + 1)
    tallies = tallies.at[1:1 + 2 * couples:2].set(donor - moved).at[2:2 + 2 * couples:2].set(receiver + moved)
    return tallies[jax.random.permutation(jax.random.fold_in(rng, 2), amount)]


def gaussian(stream_key, dims, scale, most, split=(), held_as=jnp.bfloat16):
    result = scale * jax.random.normal(stream_key, dims, jnp.float32)
    if split:
        result = result * block_levels(stream_key, dims, split, -0.22, 0.18)
    return jnp.clip(result, -most, most).astype(held_as)


def setup_inputs(seed: int = 0) -> dict:
    key_of = jax.random.split(jax.random.key(seed), 18)
    return {
        "piece_tokens": gaussian(key_of[0], (PIECE, D), 1.0, 6.0, ((0, 8),)),
        "decode_tokens": gaussian(key_of[1], (DEC, D), 1.0, 6.0, ((0, 8),)),
        "prompt_fill": jax.random.randint(key_of[2], (1,), CACHE // 2, CACHE - PIECE + 1).astype(jnp.int32),
        "decode_fill": uneven(key_of[3], DEC, DEC * DEC_LEN // 2, DEC_LEN - 1, 2).astype(jnp.int32),
        "prompt_cache": draw_prompt_cache(jax.random.fold_in(key_of[17], 71), 0),
        "decode_cache": draw_decode_cache(jax.random.fold_in(key_of[17], 71), 0),
        "input_gain": jnp.clip(1.0 + 0.18 * jax.random.normal(key_of[6], (D,), jnp.float32), 0.1, 1.9),
        "query_gain": jnp.clip(1.0 + 0.18 * jax.random.normal(key_of[7], (QL,), jnp.float32), 0.1, 1.9),
        "latent_gain": jnp.clip(1.0 + 0.18 * jax.random.normal(key_of[8], (KL,), jnp.float32), 0.1, 1.9),
        "query_down": gaussian(key_of[9], (D, QL), D ** -0.5, 0.125, ((1, 4),)),
        "latent_down": gaussian(key_of[10], (D, KL), D ** -0.5, 0.125, ((1, 4),)),
        "rope_down": gaussian(key_of[11], (D, ROPE), D ** -0.5, 0.125),
        "query_up": gaussian(key_of[12], (QL, H * NOPE), QL ** -0.5, 0.21875, ((1, 4),)),
        "qrope_up": gaussian(key_of[13], (QL, H * ROPE), QL ** -0.5, 0.21875, ((1, 4),)),
        "key_up": gaussian(key_of[14], (H, NOPE, KL), KL ** -0.5, 0.25, ((0, 4),)),
        "value_up": gaussian(key_of[15], (H, KL, VD), 0.25, 4.0, ((0, 4),)),
        "out_proj": gaussian(key_of[16], (H * VD, D), 0.25, 4.0, ((0, 4),)),
    }


NEG_FILL = -1e+30
RMS_EPS = 1e-06
THETA = 10000.0

def rms_scale(values, gain_row):
    widened = values.astype(jnp.float32)
    scaled = widened * lax.rsqrt(lax.optimization_barrier(jnp.mean(widened * widened, axis=-1, keepdims=True)) + RMS_EPS) * gain_row.astype(jnp.float32)
    return scaled.astype(jnp.bfloat16)

def rotate(values, places):
    half_width = values.shape[-1] // 2
    inverse = THETA ** (-jnp.arange(half_width, dtype=jnp.float32) / half_width)
    angles = places.astype(jnp.float32)[..., None] * inverse
    first_half = values[..., :half_width].astype(jnp.float32)
    second_half = values[..., half_width:].astype(jnp.float32)
    cosine = jnp.cos(angles)
    sine_part = jnp.sin(angles)
    return jnp.concatenate([first_half * cosine - second_half * sine_part, first_half * sine_part + second_half * cosine], axis=-1).astype(jnp.bfloat16)

def project(tokens, places, input_gain, query_gain, latent_gain, query_down, latent_down, rope_down):
    normed = rms_scale(tokens, input_gain)
    query_comp = jnp.dot(normed, query_down, preferred_element_type=jnp.float32).astype(jnp.bfloat16)
    latent_comp = jnp.dot(normed, latent_down, preferred_element_type=jnp.float32).astype(jnp.bfloat16)
    rope_raw = jnp.dot(normed, rope_down, preferred_element_type=jnp.float32).astype(jnp.bfloat16)
    new_rows = jnp.concatenate([rms_scale(latent_comp, latent_gain), rotate(rope_raw, places)], axis=-1)
    return (rms_scale(query_comp, query_gain), new_rows)

def make_queries(query_lat, places, query_up, qrope_up, key_up):
    row_count = query_lat.shape[0]
    head_count = key_up.shape[0]
    nope_part = jnp.dot(query_lat, query_up, preferred_element_type=jnp.float32).astype(jnp.bfloat16).reshape(row_count, head_count, -1)
    rope_raw = jnp.dot(query_lat, qrope_up, preferred_element_type=jnp.float32).astype(jnp.bfloat16).reshape(row_count, head_count, -1)
    turned = rotate(rope_raw, places[:, None])
    absorbed = jnp.einsum('nhc,hcl->nhl', nope_part.astype(jnp.float32), key_up.astype(jnp.float32)).astype(jnp.bfloat16)
    return (absorbed, turned)

def block_attend(absorbed, turned, key_rows, key_places, query_places, value_up):
    latent_width = value_up.shape[1]
    score_scale = (NOPE + ROPE) ** (-0.5)
    latent_keys = key_rows[:, :latent_width].astype(jnp.float32)
    scores = (jnp.einsum('nhl,sl->nhs', absorbed.astype(jnp.float32), latent_keys) + jnp.einsum('nhr,sr->nhs', turned.astype(jnp.float32), key_rows[:, latent_width:].astype(jnp.float32))) * score_scale
    allowed = key_places[None, None, :] <= query_places[:, None, None]
    scores = jnp.where(allowed, scores, NEG_FILL)
    local_peak = lax.optimization_barrier(jnp.max(scores, axis=-1))
    exp_scores = jnp.where(allowed, jnp.exp(scores - local_peak[..., None]), 0.0)
    weight_sum = lax.optimization_barrier(jnp.sum(exp_scores, axis=-1))
    weights = lax.optimization_barrier(exp_scores.astype(jnp.bfloat16)).astype(jnp.float32)
    mixed_rows = jnp.einsum('nhs,sl->nhl', weights, latent_keys)
    partial_sum = jnp.einsum('nhl,hlv->nhv', mixed_rows, value_up.astype(jnp.float32), precision=lax.Precision.HIGHEST)
    return (partial_sum, weight_sum, local_peak)

def insert_row(cache_rows, new_row, fill_one):
    return lax.dynamic_update_slice(cache_rows, new_row[None], (fill_one.astype(jnp.int32), jnp.zeros((), jnp.int32)))

def project_out(values, out_proj):
    row_count = values.shape[0]
    grouped = values.reshape(row_count, N_TP, -1).astype(jnp.float32)
    weight_groups = out_proj.reshape(N_TP, -1, out_proj.shape[1]).astype(jnp.float32)
    group_out = jnp.einsum('ngk,gkd->ngd', grouped, weight_groups).astype(jnp.bfloat16)
    group_out = lax.optimization_barrier(group_out).astype(jnp.float32)
    return lax.optimization_barrier(jnp.sum(group_out, axis=1)).astype(jnp.bfloat16)

def reference(piece_tokens, decode_tokens, prompt_fill, decode_fill, prompt_cache, decode_cache, input_gain, query_gain, latent_gain, query_down, latent_down, rope_down, query_up, qrope_up, key_up, value_up, out_proj):
    fill_start = prompt_fill[0].astype(jnp.int32)
    piece_places = fill_start + jnp.arange(PIECE, dtype=jnp.int32)
    decode_places = decode_fill.astype(jnp.int32)
    piece_lat, piece_rows = project(piece_tokens, piece_places, input_gain, query_gain, latent_gain, query_down, latent_down, rope_down)
    decode_lat, decode_rows = project(decode_tokens, decode_places, input_gain, query_gain, latent_gain, query_down, latent_down, rope_down)
    piece_absorbed, piece_turned = make_queries(piece_lat, piece_places, query_up, qrope_up, key_up)
    decode_absorbed, decode_turned = make_queries(decode_lat, decode_places, query_up, qrope_up, key_up)
    full_cache = lax.dynamic_update_slice(prompt_cache, piece_rows, (fill_start, jnp.zeros((), jnp.int32)))
    head_count = key_up.shape[0]
    value_width = value_up.shape[2]

    def step(carry, block_index):
        peak_run, numer_run, denom_run = carry
        key_rows = lax.dynamic_slice_in_dim(full_cache, block_index * CACHE_DEV, CACHE_DEV, 0)
        key_places = block_index * CACHE_DEV + jnp.arange(CACHE_DEV, dtype=jnp.int32)
        partial_sum, weight_sum, local_peak = block_attend(piece_absorbed, piece_turned, key_rows, key_places, piece_places, value_up)
        new_peak = jnp.maximum(peak_run, local_peak)
        old_factor = jnp.exp(peak_run - new_peak)
        new_factor = jnp.exp(local_peak - new_peak)
        numer_run = numer_run * old_factor[..., None] + partial_sum * new_factor[..., None]
        denom_run = denom_run * old_factor + weight_sum * new_factor
        return ((new_peak, numer_run, denom_run), None)
    start_carry = (jnp.full((PIECE, head_count), NEG_FILL, jnp.float32), jnp.zeros((PIECE, head_count, value_width), jnp.float32), jnp.zeros((PIECE, head_count), jnp.float32))
    final_carry, unused = lax.scan(step, start_carry, jnp.arange(N_KV, dtype=jnp.int32))
    piece_value = (final_carry[1] / final_carry[2][..., None]).astype(jnp.bfloat16)
    decode_keys = jax.vmap(insert_row)(decode_cache, decode_rows, decode_places)

    def attend_one(absorbed_one, turned_one, keys_one, fill_one):
        key_places = jnp.arange(keys_one.shape[0], dtype=jnp.int32)
        return block_attend(absorbed_one[None], turned_one[None], keys_one, key_places, fill_one[None], value_up)
    decode_part, decode_total, decode_peak = jax.vmap(attend_one)(decode_absorbed, decode_turned, decode_keys, decode_places)
    decode_value = (decode_part[:, 0] / decode_total[:, 0, :, None]).astype(jnp.bfloat16)
    piece_out = project_out(piece_value.reshape(PIECE, -1), out_proj)
    decode_out = project_out(decode_value.reshape(decode_value.shape[0], -1), out_proj)
    return (piece_out, decode_out, piece_rows, decode_rows)
```

```python
import functools
import math

import jax
import jax.numpy as jnp
from jax import lax
from jax.experimental import pallas as pl
from jax.experimental.pallas import tpu as pltpu
from jax.sharding import PartitionSpec as P

NOPE = 64
ROPE = 32
NEG_FILL = -1e30
RMS_EPS = 1e-06
THETA = 10000.0
F32 = jnp.float32
BF16 = jnp.bfloat16
MESH = pl.DeviceIdType.MESH


def dot(a, b):
    return jnp.dot(a, b, preferred_element_type=F32)


def dot_t(a, b):
    return lax.dot_general(a, b, (((1,), (1,)), ((), ())), preferred_element_type=F32)


def round_up(value, step):
    return -(-value // step) * step


def kernel(
    n,
    m,
    pt_h,
    dt_h,
    pfill,
    dfill,
    pc_h,
    dc_h,
    ig_h,
    qg_h,
    lg_h,
    qd_h,
    ld_h,
    rd_h,
    qu_h,
    ru_h,
    ku_h,
    vu_h,
    op_h,
    po_ref,
    do_ref,
    pr_ref,
    dr_ref,
    tok,
    dtok,
    kbuf,
    dbuf,
    ig,
    qg,
    lg,
    qd,
    ld,
    rd,
    qu,
    ru,
    ku,
    vu,
    op,
    x,
    qx,
    lx,
    csend,
    crecv,
    vbuf,
    obuf,
    in_sem,
    tok_sem,
    a_sem,
    l_sem,
    c_sem,
    o_sem,
):
    me = lax.axis_index("kv")
    mt = lax.axis_index("tp")
    p = tok.shape[1]
    dd = dtok.shape[0]
    width = tok.shape[2]
    own = vbuf.shape[0]
    rows = x.shape[0]
    cache = pc_h.shape[0]
    slots = dc_h.shape[1]
    heads = ku.shape[0]
    kl = ku.shape[2]
    key_width = kbuf.shape[1]
    part_q = qd.shape[1]
    ql = qu.shape[0]
    extra = kbuf.shape[0] - cache
    chunk = obuf.shape[3]
    chunks = obuf.shape[1]

    pairs = [
        (pt_h, tok.at[0]),
        (dt_h, dtok),
        (ig_h, ig),
        (qd_h, qd),
        (ld_h, ld),
        (rd_h, rd),
        (qg_h, qg),
        (lg_h, lg),
        (qu_h, qu),
        (ru_h, ru),
        (ku_h, ku),
        (pc_h, kbuf.at[pl.ds(0, cache)]),
        (vu_h, vu),
        (dc_h, dbuf.at[:, pl.ds(0, slots)]),
        (op_h, op),
    ]
    loads = [pltpu.make_async_copy(s, d, in_sem.at[i]) for i, (s, d) in enumerate(pairs)]
    for load in loads:
        load.start()
    l_pt, l_dt, l_ig, l_qd, l_ld, l_rd, l_qg, l_lg, l_qu, l_ru, l_ku, l_pc, l_vu, l_dc, l_op = loads

    barrier = pltpu.get_barrier_semaphore()
    for d in range(1, n):
        pl.semaphore_signal(
            barrier, inc=1, device_id=(lax.rem(me + d, n), mt), device_id_type=MESH
        )
    for d in range(1, m):
        pl.semaphore_signal(
            barrier, inc=1, device_id=(me, lax.rem(mt + d, m)), device_id_type=MESH
        )
    l_pt.wait()
    pl.semaphore_wait(barrier, n - 1 + m - 1)

    tok_copies = []
    for d in range(1, n):
        copy = pltpu.make_async_remote_copy(
            src_ref=tok.at[0],
            dst_ref=tok.at[d],
            send_sem=tok_sem.at[0, d],
            recv_sem=tok_sem.at[1, d],
            device_id=(lax.rem(me + d, n), mt),
            device_id_type=MESH,
        )
        copy.start()
        tok_copies.append(copy)

    fill = pfill[0]
    row = lax.broadcasted_iota(jnp.int32, (rows, 1), 0)
    slot = jnp.zeros((rows, 1), jnp.int32)
    for d in range(1, n):
        slot = jnp.where(row >= own + (d - 1) * p, d, slot)
    source = me - slot
    source = jnp.where(source < 0, source + n, source)
    inside = jnp.where(slot == 0, row, row - own - (slot - 1) * p)
    places = fill + source * p + inside
    for b in range(dd):
        places = jnp.where(row == p + b, dfill[b], places)
    half = ROPE // 2
    lane = lax.broadcasted_iota(jnp.int32, (1, heads * ROPE), 1)
    frequency = jnp.zeros((1, heads * ROPE), F32)
    for i in range(half):
        frequency = jnp.where(lane % half == i, THETA ** (-i / half), frequency)
    angles = places.astype(F32) * frequency
    cosine = jnp.cos(angles)
    sine = jnp.sin(angles)

    x[...] = jnp.zeros_like(x)
    x[0:p, :] = tok[0].astype(F32)
    l_dt.wait()
    x[p : p + dd, :] = dtok[...].astype(F32)
    l_ig.wait()
    l_qd.wait()
    l_ld.wait()
    l_rd.wait()
    for d in range(1, n):
        tok_copies[d - 1].wait_recv()
        start = own + (d - 1) * p
        x[start : start + p, :] = tok[d].astype(F32)
    xs = x[...]
    normed = (
        xs * lax.rsqrt(jnp.mean(xs * xs, axis=-1, keepdims=True) + RMS_EPS) * ig[...]
    ).astype(BF16)
    qx[mt] = dot(normed, qd[...]).astype(BF16)
    lx[mt] = dot(normed[0:extra], ld[...]).astype(BF16)

    a_copies = []
    for d in range(1, m):
        peer = (me, lax.rem(mt + d, m))
        for buf, sem in ((qx, a_sem), (lx, l_sem)):
            copy = pltpu.make_async_remote_copy(
                src_ref=buf.at[mt],
                dst_ref=buf.at[mt],
                send_sem=sem.at[0, d],
                recv_sem=sem.at[1, d],
                device_id=peer,
                device_id_type=MESH,
            )
            copy.start()
            a_copies.append(copy)

    raw = dot(normed[0:extra], rd[...]).astype(BF16).astype(F32)
    cos_own = cosine[0:extra, 0:half]
    sin_own = sine[0:extra, 0:half]
    first, second = raw[:, 0:half], raw[:, half:ROPE]
    new_rope = jnp.concatenate(
        [first * cos_own - second * sin_own, first * sin_own + second * cos_own], axis=1
    )
    for load in (l_qg, l_lg, l_qu, l_ru, l_ku, l_pc, l_vu, l_dc):
        load.wait()
    gains = qg[...]
    for copy in a_copies:
        copy.wait_recv()

    parts = [qx[s].astype(F32) for s in range(m)]
    square = sum(jnp.sum(v * v, axis=-1, keepdims=True) for v in parts)
    scale = lax.rsqrt(square / ql + RMS_EPS)
    nope = jnp.zeros((rows, qu.shape[1]), F32)
    turn = jnp.zeros((rows, ru.shape[1]), F32)
    for s in range(m):
        lat = (parts[s] * scale * gains[:, s * part_q : (s + 1) * part_q]).astype(BF16)
        nope += dot(lat, qu[s * part_q : (s + 1) * part_q, :])
        turn += dot(lat, ru[s * part_q : (s + 1) * part_q, :])
    nope = nope.astype(BF16)
    turn = turn.astype(BF16).astype(F32)
    turned_axis = heads * ROPE
    above = pltpu.roll(turn, turned_axis - half, 1)
    below = pltpu.roll(turn, half, 1)
    turned = turn * cosine + jnp.where(lane % ROPE < half, -above, below) * sine
    nd = qu.shape[1] // heads
    absorbed = [dot(nope[:, h * nd : (h + 1) * nd], ku[h]) for h in range(heads)]
    turned = [turned[:, h * ROPE : (h + 1) * ROPE] for h in range(heads)]

    latent = jnp.concatenate([lx[s].astype(F32) for s in range(m)], axis=1)
    latent = (
        latent * lax.rsqrt(jnp.mean(latent * latent, axis=-1, keepdims=True) + RMS_EPS) * lg[...]
    )
    new_rows = jnp.concatenate([latent, new_rope], axis=1)
    new_bf = new_rows.astype(BF16)
    kbuf[cache : cache + extra, :] = new_bf
    pr_ref[...] = new_rows[0:p].astype(BF16)
    dr_ref[...] = new_rows[p : p + dd].astype(BF16)

    score_scale = (NOPE + ROPE) ** (-0.5)
    aq = jnp.concatenate([v.astype(BF16) for v in absorbed], axis=0)
    tq = jnp.concatenate([v.astype(BF16) for v in turned], axis=0)
    scores = (dot_t(aq, kbuf[:, 0:kl]) + dot_t(tq, kbuf[:, kl:key_width])) * score_scale
    key = lax.broadcasted_iota(jnp.int32, scores.shape, 1)
    query_place = jnp.concatenate([places] * heads, axis=0)
    fresh = key - cache
    key_place = jnp.where(fresh < 0, me * cache + key, fill + me * p + fresh)
    limit = jnp.where(fresh < 0, jnp.minimum(fill - 1, query_place), query_place)
    allowed = (key_place <= limit) & (fresh < p)
    scores = jnp.where(allowed, scores, NEG_FILL)
    peak = jnp.max(scores, axis=-1, keepdims=True)
    weights = jnp.where(allowed, jnp.exp(scores - peak), 0.0)
    total = jnp.sum(weights, axis=-1, keepdims=True)
    mixed = dot(weights.astype(BF16), kbuf[:, 0:kl]).astype(BF16)
    vd = vu.shape[2]
    stat_lane = lax.broadcasted_iota(jnp.int32, (rows, crecv.shape[2] - vd), 1)
    for h in range(heads):
        cut = slice(h * rows, (h + 1) * rows)
        stats = jnp.where(stat_lane == 0, total[cut], peak[cut])
        message = jnp.concatenate([dot(mixed[cut], vu[h]), stats], axis=1)
        csend[0, h * p : (h + 1) * p, :] = message[0:p]
        for d in range(1, n):
            start = own + (d - 1) * p
            csend[d, h * p : (h + 1) * p, :] = message[start : start + p]

    c_copies = []
    for d in range(1, n):
        copy = pltpu.make_async_remote_copy(
            src_ref=csend.at[d],
            dst_ref=crecv.at[d],
            send_sem=c_sem.at[0, d],
            recv_sem=c_sem.at[1, d],
            device_id=(lax.rem(me + n - d, n), mt),
            device_id_type=MESH,
        )
        copy.start()
        c_copies.append(copy)

    vbuf[...] = jnp.zeros_like(vbuf)
    for b in range(dd):
        dbuf[b, slots : slots + extra, :] = new_bf
        at = slice(p + b, p + b + 1)
        qa = jnp.concatenate([v[at] for v in absorbed], axis=0).astype(BF16)
        qt = jnp.concatenate([v[at] for v in turned], axis=0).astype(BF16)
        ds = (dot_t(qa, dbuf[b, :, 0:kl]) + dot_t(qt, dbuf[b, :, kl:key_width])) * score_scale
        dk = lax.broadcasted_iota(jnp.int32, ds.shape, 1)
        ok = (dk < jnp.minimum(dfill[b], slots)) | (dk == slots + p + b)
        ds = jnp.where(ok, ds, NEG_FILL)
        dpeak = jnp.max(ds, axis=-1, keepdims=True)
        dw = jnp.where(ok, jnp.exp(ds - dpeak), 0.0)
        dtotal = jnp.sum(dw, axis=-1, keepdims=True)
        dmix = dot(dw.astype(BF16), dbuf[b, :, 0:kl]).astype(BF16)
        dvals = [dot(dmix, vu[h])[h : h + 1] / dtotal[h : h + 1] for h in range(heads)]
        vbuf[p + b : p + b + 1, :] = jnp.concatenate(dvals, axis=1)
    l_op.wait()

    for copy in c_copies:
        copy.wait_recv()
    blocks = [csend[0]] + [crecv[d] for d in range(1, n)]
    top = blocks[0][:, vd + 1 : vd + 2]
    for block in blocks[1:]:
        top = jnp.maximum(top, block[:, vd + 1 : vd + 2])
    merged = jnp.zeros(blocks[0].shape, F32)
    for block in blocks:
        merged += block * jnp.exp(block[:, vd + 1 : vd + 2] - top)
    value = merged[:, 0:vd] / merged[:, vd : vd + 1]
    vbuf[0:p, :] = jnp.concatenate([value[h * p : (h + 1) * p] for h in range(heads)], axis=1)
    values = vbuf[...].astype(BF16)

    o_copies = []
    for c in range(chunks):
        obuf[mt, c] = dot(values, op[:, c * chunk : (c + 1) * chunk]).astype(BF16)
        for d in range(1, m):
            copy = pltpu.make_async_remote_copy(
                src_ref=obuf.at[mt, c],
                dst_ref=obuf.at[mt, c],
                send_sem=o_sem.at[0, d, c],
                recv_sem=o_sem.at[1, d, c],
                device_id=(me, lax.rem(mt + d, m)),
                device_id_type=MESH,
            )
            copy.start()
            o_copies.append(copy)
    for copy in o_copies:
        copy.wait_recv()
    for c in range(chunks):
        out = sum(obuf[s, c].astype(F32) for s in range(m))
        po_ref[:, c * chunk : (c + 1) * chunk] = out[0:p].astype(BF16)
        do_ref[:, c * chunk : (c + 1) * chunk] = out[p : p + dd].astype(BF16)
    for copy in tok_copies + a_copies + c_copies + o_copies:
        copy.wait_send()


def local(n, m, *args):
    (pt, dt, pfill, dfill, pc, dc, ig, qg, lg, qd, ld, rd, qu, ru, ku, vu, op) = args
    p, width = pt.shape
    dd = dt.shape[0]
    own = round_up(p + dd, 8)
    rows = round_up(own + (n - 1) * p, 16)
    extra = round_up(own, 16)
    heads, nd, kl = ku.shape
    chunks = 2
    any_spec = pl.BlockSpec(memory_space=pl.ANY)
    smem = pl.BlockSpec(memory_space=pltpu.SMEM)
    vmem = pl.BlockSpec(memory_space=pltpu.VMEM)
    ig, qg, lg = ig[None], qg[None], lg[None]
    like = lambda a: pltpu.VMEM(a.shape, a.dtype)
    scratch = [
        pltpu.VMEM((n, p, width), BF16),
        like(dt),
        pltpu.VMEM((pc.shape[0] + extra, pc.shape[1]), BF16),
        pltpu.VMEM((dd, dc.shape[1] + extra, dc.shape[2]), BF16),
        *[like(a) for a in (ig, qg, lg, qd, ld, rd, qu, ru, ku, vu, op)],
        pltpu.VMEM((rows, width), F32),
        pltpu.VMEM((m, rows, qd.shape[1]), BF16),
        pltpu.VMEM((m, extra, ld.shape[1]), BF16),
        pltpu.VMEM((n, heads * p, 128), F32),
        pltpu.VMEM((n, heads * p, 128), F32),
        pltpu.VMEM((own, op.shape[0]), F32),
        pltpu.VMEM((m, chunks, own, width // chunks), BF16),
        pltpu.SemaphoreType.DMA((15,)),
        pltpu.SemaphoreType.DMA((2, n)),
        pltpu.SemaphoreType.DMA((2, m)),
        pltpu.SemaphoreType.DMA((2, m)),
        pltpu.SemaphoreType.DMA((2, n)),
        pltpu.SemaphoreType.DMA((2, m, chunks)),
    ]
    return pl.pallas_call(
        functools.partial(kernel, n, m),
        out_shape=(
            jax.ShapeDtypeStruct((p, width), BF16),
            jax.ShapeDtypeStruct((dd, width), BF16),
            jax.ShapeDtypeStruct((p, pc.shape[1]), BF16),
            jax.ShapeDtypeStruct((dd, pc.shape[1]), BF16),
        ),
        in_specs=[any_spec, any_spec, smem, smem] + [any_spec] * 13,
        out_specs=(vmem,) * 4,
        scratch_shapes=scratch,
        compiler_params=pltpu.CompilerParams(
            collective_id=0, has_side_effects=True, vmem_limit_bytes=60 * 1024 * 1024
        ),
    )(pt, dt, pfill, dfill, pc, dc, ig, qg, lg, qd, ld, rd, qu, ru, ku, vu, op)


def solution(mesh):
    placed = (
        P("kv", None),
        P("kv", None),
        P(),
        P("kv"),
        P("kv", None),
        P("kv", None, None),
        P(),
        P(),
        P(),
        P(None, "tp"),
        P(None, "tp"),
        P(),
        P(None, "tp"),
        P(None, "tp"),
        P("tp", None, None),
        P("tp", None, None),
        P("tp", None),
    )
    return jax.shard_map(
        functools.partial(local, mesh.shape["kv"], mesh.shape["tp"]),
        mesh=mesh,
        in_specs=placed,
        out_specs=(P("kv", None), P("kv", None), P("kv", None), P("kv", None)),
        check_vma=False,
    )
```

```python
import functools
import math

import jax
import jax.numpy as jnp
from jax import lax
from jax.experimental import pallas as pl
from jax.experimental.pallas import tpu as pltpu
from jax.sharding import PartitionSpec as P

NOPE = 64
ROPE = 32
NEG_FILL = -1e30
RMS_EPS = 1e-06
THETA = 10000.0
F32 = jnp.float32
BF16 = jnp.bfloat16
MESH = pl.DeviceIdType.MESH


def dot(a, b):
    return jnp.dot(a, b, preferred_element_type=F32)


def dot_t(a, b):
    return lax.dot_general(a, b, (((1,), (1,)), ((), ())), preferred_element_type=F32)


def round_up(value, step):
    return -(-value // step) * step


def kernel(
    n,
    m,
    pt_h,
    dt_h,
    pf_h,
    df_h,
    pc_h,
    dc_h,
    ig_h,
    qg_h,
    lg_h,
    qd_h,
    ld_h,
    rd_h,
    qu_h,
    ru_h,
    ku_h,
    vu_h,
    op_h,
    po_ref,
    do_ref,
    pr_ref,
    dr_ref,
    tok,
    dtok,
    pfill,
    dfill,
    kbuf,
    dbuf,
    ig,
    qg,
    lg,
    qd,
    ld,
    rd,
    qu,
    ru,
    ku,
    vu,
    op,
    x,
    qx,
    lx,
    csend,
    crecv,
    vbuf,
    obuf,
    in_sem,
    tok_sem,
    a_sem,
    l_sem,
    c_sem,
    o_sem,
):
    me = lax.axis_index("kv")
    mt = lax.axis_index("tp")
    p = tok.shape[1]
    dd = dtok.shape[0]
    width = tok.shape[2]
    own = vbuf.shape[0]
    rows = x.shape[0]
    cache = pc_h.shape[1]
    slots = dc_h.shape[2]
    heads = ku.shape[0]
    kl = ku.shape[2]
    key_width = kbuf.shape[0]
    part_q = qd.shape[0]
    ql = qu.shape[0]
    extra = lx.shape[1]
    chunk = obuf.shape[3]
    chunks = obuf.shape[1]

    pairs = [
        (pt_h, tok.at[0]),
        (dt_h, dtok),
        (pf_h, pfill),
        (df_h, dfill),
        (ig_h, ig),
        (qd_h, qd),
        (ld_h, ld),
        (rd_h, rd),
        (qg_h, qg),
        (lg_h, lg),
        (qu_h, qu),
        (ru_h, ru),
        (ku_h, ku),
        (pc_h, kbuf),
        (vu_h, vu),
        (dc_h, dbuf),
        (op_h, op),
    ]
    loads = [pltpu.make_async_copy(s, d, in_sem.at[i]) for i, (s, d) in enumerate(pairs)]
    for load in loads:
        load.start()
    l_pt, l_dt, l_pf, l_df, l_ig, l_qd, l_ld, l_rd, l_qg, l_lg, l_qu, l_ru, l_ku, l_pc, l_vu, l_dc, l_op = loads

    barrier = pltpu.get_barrier_semaphore()
    for d in range(1, n):
        pl.semaphore_signal(
            barrier, inc=1, device_id=(lax.rem(me + d, n), mt), device_id_type=MESH
        )
    for d in range(1, m):
        pl.semaphore_signal(
            barrier, inc=1, device_id=(me, lax.rem(mt + d, m)), device_id_type=MESH
        )
    l_pt.wait()
    pl.semaphore_wait(barrier, n - 1 + m - 1)

    tok_copies = []
    for d in range(1, n):
        copy = pltpu.make_async_remote_copy(
            src_ref=tok.at[0],
            dst_ref=tok.at[d],
            send_sem=tok_sem.at[0, d],
            recv_sem=tok_sem.at[1, d],
            device_id=(lax.rem(me + d, n), mt),
            device_id_type=MESH,
        )
        copy.start()
        tok_copies.append(copy)

    l_pf.wait()
    l_df.wait()
    fill = pfill[0]
    row = lax.broadcasted_iota(jnp.int32, (rows, 1), 0)
    slot = jnp.zeros((rows, 1), jnp.int32)
    for d in range(1, n):
        slot = jnp.where(row >= own + (d - 1) * p, d, slot)
    source = me - slot
    source = jnp.where(source < 0, source + n, source)
    inside = jnp.where(slot == 0, row, row - own - (slot - 1) * p)
    places = fill + source * p + inside
    for b in range(dd):
        places = jnp.where(row == p + b, dfill[b], places)
    half = ROPE // 2
    lane = lax.broadcasted_iota(jnp.int32, (1, heads * ROPE), 1)
    frequency = jnp.zeros((1, heads * ROPE), F32)
    for i in range(half):
        frequency = jnp.where(lane % half == i, THETA ** (-i / half), frequency)
    angles = places.astype(F32) * frequency
    cosine = jnp.cos(angles)
    sine = jnp.sin(angles)

    x[...] = jnp.zeros_like(x)
    x[0:p, :] = tok[0].astype(F32)
    l_dt.wait()
    x[p : p + dd, :] = dtok[...].astype(F32)
    l_ig.wait()
    l_qd.wait()
    l_ld.wait()
    l_rd.wait()
    for d in range(1, n):
        tok_copies[d - 1].wait_recv()
        start = own + (d - 1) * p
        x[start : start + p, :] = tok[d].astype(F32)
    xs = x[...]
    normed = (
        xs * lax.rsqrt(jnp.mean(xs * xs, axis=-1, keepdims=True) + RMS_EPS) * ig[...]
    ).astype(BF16)
    qx[mt] = dot_t(normed, qd[...]).astype(BF16)
    lx[mt] = dot(normed[0:extra], ld[...]).astype(BF16)

    a_copies = []
    for d in range(1, m):
        peer = (me, lax.rem(mt + d, m))
        for buf, sem in ((qx, a_sem), (lx, l_sem)):
            copy = pltpu.make_async_remote_copy(
                src_ref=buf.at[mt],
                dst_ref=buf.at[mt],
                send_sem=sem.at[0, d],
                recv_sem=sem.at[1, d],
                device_id=peer,
                device_id_type=MESH,
            )
            copy.start()
            a_copies.append(copy)

    raw = dot_t(normed[0:extra], rd[...]).astype(BF16).astype(F32)
    cos_own = cosine[0:extra, 0:half]
    sin_own = sine[0:extra, 0:half]
    first, second = raw[:, 0:half], raw[:, half:ROPE]
    new_rope = jnp.concatenate(
        [first * cos_own - second * sin_own, first * sin_own + second * cos_own], axis=1
    )
    for load in (l_qg, l_lg, l_qu, l_ru, l_ku, l_pc, l_vu, l_dc):
        load.wait()
    gains = qg[...].reshape(1, ql)
    for copy in a_copies:
        copy.wait_recv()

    parts = [qx[s].astype(F32) for s in range(m)]
    square = sum(jnp.sum(v * v, axis=-1, keepdims=True) for v in parts)
    scale = lax.rsqrt(square / ql + RMS_EPS)
    nope = jnp.zeros((rows, qu.shape[1]), F32)
    turn = jnp.zeros((rows, ru.shape[1]), F32)
    for s in range(m):
        lat = (parts[s] * scale * gains[:, s * part_q : (s + 1) * part_q]).astype(BF16)
        nope += dot(lat, qu[s * part_q : (s + 1) * part_q, :])
        turn += dot(lat, ru[s * part_q : (s + 1) * part_q, :])
    nope = nope.astype(BF16)
    turn = turn.astype(BF16).astype(F32)
    turned_axis = heads * ROPE
    above = pltpu.roll(turn, turned_axis - half, 1)
    below = pltpu.roll(turn, half, 1)
    turned = turn * cosine + jnp.where(lane % ROPE < half, -above, below) * sine
    nd = qu.shape[1] // heads
    absorbed = [dot(nope[:, h * nd : (h + 1) * nd], ku[h]) for h in range(heads)]
    turned = [turned[:, h * ROPE : (h + 1) * ROPE] for h in range(heads)]

    latent = jnp.concatenate([lx[s].astype(F32) for s in range(m)], axis=1)
    latent = (
        latent * lax.rsqrt(jnp.mean(latent * latent, axis=-1, keepdims=True) + RMS_EPS) * lg[...]
    )
    new_rows = jnp.concatenate([latent, new_rope], axis=1)
    new_bf = new_rows.astype(BF16)
    new_latent, new_key = new_bf[:, 0:kl], new_bf[:, kl:key_width]
    pr_ref[...] = new_rows[0:p].astype(BF16)
    dr_ref[...] = new_rows[p : p + dd].astype(BF16)

    score_scale = (NOPE + ROPE) ** (-0.5)
    aq = jnp.concatenate([v.astype(BF16) for v in absorbed], axis=0)
    tq = jnp.concatenate([v.astype(BF16) for v in turned], axis=0)
    scores = (
        jnp.concatenate(
            [
                dot(aq, kbuf[0:kl]) + dot(tq, kbuf[kl:key_width]),
                dot_t(aq, new_latent) + dot_t(tq, new_key),
            ],
            axis=1,
        )
        * score_scale
    )
    key = lax.broadcasted_iota(jnp.int32, scores.shape, 1)
    query_place = jnp.concatenate([places] * heads, axis=0)
    fresh = key - cache
    key_place = jnp.where(fresh < 0, me * cache + key, fill + me * p + fresh)
    limit = jnp.where(fresh < 0, jnp.minimum(fill - 1, query_place), query_place)
    allowed = (key_place <= limit) & (fresh < p)
    scores = jnp.where(allowed, scores, NEG_FILL)
    peak = jnp.max(scores, axis=-1, keepdims=True)
    weights = jnp.where(allowed, jnp.exp(scores - peak), 0.0)
    total = jnp.sum(weights, axis=-1, keepdims=True)
    weights = weights.astype(BF16)
    mixed = (
        dot_t(weights[:, 0:cache], kbuf[0:kl]) + dot(weights[:, cache:], new_latent)
    ).astype(BF16)
    vd = vu.shape[1]
    stat_lane = lax.broadcasted_iota(jnp.int32, (rows, crecv.shape[2] - vd), 1)
    for h in range(heads):
        cut = slice(h * rows, (h + 1) * rows)
        stats = jnp.where(stat_lane == 0, total[cut], peak[cut])
        message = jnp.concatenate([dot_t(mixed[cut], vu[h]), stats], axis=1)
        csend[0, h * p : (h + 1) * p, :] = message[0:p]
        for d in range(1, n):
            start = own + (d - 1) * p
            csend[d, h * p : (h + 1) * p, :] = message[start : start + p]

    c_copies = []
    for d in range(1, n):
        copy = pltpu.make_async_remote_copy(
            src_ref=csend.at[d],
            dst_ref=crecv.at[d],
            send_sem=c_sem.at[0, d],
            recv_sem=c_sem.at[1, d],
            device_id=(lax.rem(me + n - d, n), mt),
            device_id_type=MESH,
        )
        copy.start()
        c_copies.append(copy)

    vbuf[...] = jnp.zeros_like(vbuf)
    for b in range(dd):
        at = slice(p + b, p + b + 1)
        qa = jnp.concatenate([v[at] for v in absorbed], axis=0).astype(BF16)
        qt = jnp.concatenate([v[at] for v in turned], axis=0).astype(BF16)
        ds = (
            jnp.concatenate(
                [
                    dot(qa, dbuf[b, 0:kl]) + dot(qt, dbuf[b, kl:key_width]),
                    dot_t(qa, new_latent) + dot_t(qt, new_key),
                ],
                axis=1,
            )
            * score_scale
        )
        dk = lax.broadcasted_iota(jnp.int32, ds.shape, 1)
        ok = (dk < jnp.minimum(dfill[b], slots)) | (dk == slots + p + b)
        ds = jnp.where(ok, ds, NEG_FILL)
        dpeak = jnp.max(ds, axis=-1, keepdims=True)
        dw = jnp.where(ok, jnp.exp(ds - dpeak), 0.0)
        dtotal = jnp.sum(dw, axis=-1, keepdims=True)
        dw = dw.astype(BF16)
        dmix = (dot_t(dw[:, 0:slots], dbuf[b, 0:kl]) + dot(dw[:, slots:], new_latent)).astype(BF16)
        dvals = [dot_t(dmix, vu[h])[h : h + 1] / dtotal[h : h + 1] for h in range(heads)]
        vbuf[p + b : p + b + 1, :] = jnp.concatenate(dvals, axis=1)
    l_op.wait()

    for copy in c_copies:
        copy.wait_recv()
    blocks = [csend[0]] + [crecv[d] for d in range(1, n)]
    top = blocks[0][:, vd + 1 : vd + 2]
    for block in blocks[1:]:
        top = jnp.maximum(top, block[:, vd + 1 : vd + 2])
    merged = jnp.zeros(blocks[0].shape, F32)
    for block in blocks:
        merged += block * jnp.exp(block[:, vd + 1 : vd + 2] - top)
    value = merged[:, 0:vd] / merged[:, vd : vd + 1]
    vbuf[0:p, :] = jnp.concatenate([value[h * p : (h + 1) * p] for h in range(heads)], axis=1)
    values = vbuf[...].astype(BF16)

    o_copies = []
    for c in range(chunks):
        obuf[mt, c] = dot(values, op[:, c * chunk : (c + 1) * chunk]).astype(BF16)
        for d in range(1, m):
            copy = pltpu.make_async_remote_copy(
                src_ref=obuf.at[mt, c],
                dst_ref=obuf.at[mt, c],
                send_sem=o_sem.at[0, d, c],
                recv_sem=o_sem.at[1, d, c],
                device_id=(me, lax.rem(mt + d, m)),
                device_id_type=MESH,
            )
            copy.start()
            o_copies.append(copy)
    for copy in o_copies:
        copy.wait_recv()
    for c in range(chunks):
        out = sum(obuf[s, c].astype(F32) for s in range(m))
        po_ref[:, c * chunk : (c + 1) * chunk] = out[0:p].astype(BF16)
        do_ref[:, c * chunk : (c + 1) * chunk] = out[p : p + dd].astype(BF16)
    for copy in tok_copies + a_copies + c_copies + o_copies:
        copy.wait_send()


def local(n, m, *args):
    (pt, dt, pfill, dfill, pc, dc, ig, qg, lg, qd, ld, rd, qu, ru, ku, vu, op) = args
    p, width = pt.shape
    dd = dt.shape[0]
    own = round_up(p + dd, 8)
    rows = round_up(own + (n - 1) * p, 16)
    extra = round_up(own, 16)
    heads, nd, kl = ku.shape
    chunks = 2
    any_spec = pl.BlockSpec(memory_space=pltpu.HBM)
    vmem = pl.BlockSpec(memory_space=pltpu.VMEM)
    ig, lg = ig[None], lg[None]
    pc, qd, rd = pc.T, qd.T, rd.T
    dc, vu = jnp.swapaxes(dc, 1, 2), jnp.swapaxes(vu, 1, 2)
    like = lambda a: pltpu.VMEM(a.shape, a.dtype)
    scratch = [
        pltpu.VMEM((n, p, width), BF16),
        like(dt),
        pltpu.SMEM(pfill.shape, jnp.int32),
        pltpu.SMEM(dfill.shape, jnp.int32),
        *[like(a) for a in (pc, dc, ig, qg, lg, qd, ld, rd, qu, ru, ku, vu, op)],
        pltpu.VMEM((rows, width), F32),
        pltpu.VMEM((m, rows, qd.shape[0]), BF16),
        pltpu.VMEM((m, extra, ld.shape[1]), BF16),
        pltpu.VMEM((n, heads * p, 128), F32),
        pltpu.VMEM((n, heads * p, 128), F32),
        pltpu.VMEM((own, op.shape[0]), F32),
        pltpu.VMEM((m, chunks, own, width // chunks), BF16),
        pltpu.SemaphoreType.DMA((17,)),
        pltpu.SemaphoreType.DMA((2, n)),
        pltpu.SemaphoreType.DMA((2, m)),
        pltpu.SemaphoreType.DMA((2, m)),
        pltpu.SemaphoreType.DMA((2, n)),
        pltpu.SemaphoreType.DMA((2, m, chunks)),
    ]
    return pl.pallas_call(
        functools.partial(kernel, n, m),
        out_shape=(
            jax.ShapeDtypeStruct((p, width), BF16),
            jax.ShapeDtypeStruct((dd, width), BF16),
            jax.ShapeDtypeStruct((p, pc.shape[0]), BF16),
            jax.ShapeDtypeStruct((dd, pc.shape[0]), BF16),
        ),
        in_specs=[any_spec] * 17,
        out_specs=(vmem,) * 4,
        scratch_shapes=scratch,
        compiler_params=pltpu.CompilerParams(
            collective_id=0, has_side_effects=True, vmem_limit_bytes=60 * 1024 * 1024
        ),
    )(pt, dt, pfill, dfill, pc, dc, ig, qg, lg, qd, ld, rd, qu, ru, ku, vu, op)


def solution(mesh):
    placed = (
        P("kv", None),
        P("kv", None),
        P(),
        P("kv"),
        P("kv", None),
        P("kv", None, None),
        P(),
        P(),
        P(),
        P(None, "tp"),
        P(None, "tp"),
        P(),
        P(None, "tp"),
        P(None, "tp"),
        P("tp", None, None),
        P("tp", None, None),
        P("tp", None),
    )
    return jax.shard_map(
        functools.partial(local, mesh.shape["kv"], mesh.shape["tp"]),
        mesh=mesh,
        in_specs=placed,
        out_specs=(P("kv", None), P("kv", None), P("kv", None), P("kv", None)),
        check_vma=False,
    )
```

```python
import functools
import math

import jax
import jax.numpy as jnp
from jax import lax
from jax.experimental import pallas as pl
from jax.experimental.pallas import tpu as pltpu
from jax.sharding import PartitionSpec as P

NOPE = 64
ROPE = 32
NEG_FILL = -1e30
RMS_EPS = 1e-06
THETA = 10000.0
F32 = jnp.float32
BF16 = jnp.bfloat16
MESH = pl.DeviceIdType.MESH


def dot(a, b):
    return jnp.dot(a, b, preferred_element_type=F32)


def dot_t(a, b):
    return lax.dot_general(a, b, (((1,), (1,)), ((), ())), preferred_element_type=F32)


def each(low, high, body):
    if high - low <= 8:
        for i in range(low, high):
            body(i)
    else:
        lax.fori_loop(low, high, lambda i, carry: (body(i), carry)[1], 0)


def round_up(value, step):
    return -(-value // step) * step


def kernel(
    n,
    m,
    pt_h,
    dt_h,
    pf_h,
    df_h,
    pc_h,
    dc_h,
    ig_h,
    qg_h,
    lg_h,
    qd_h,
    ld_h,
    rd_h,
    qu_h,
    ru_h,
    ku_h,
    vu_h,
    op_h,
    po_ref,
    do_ref,
    pr_ref,
    dr_ref,
    tok,
    dtok,
    pfill,
    dfill,
    kbuf,
    dbuf,
    ig,
    qg,
    lg,
    qd,
    ld,
    rd,
    qu,
    ru,
    ku,
    vu,
    op,
    x,
    qall,
    lx,
    qx,
    stage,
    csend,
    crecv,
    dbuf_out,
    outs,
    in_sem,
    q_sem,
    l_sem,
    c_sem,
    d_sem,
    o_sem,
):
    me = lax.axis_index("kv")
    mt = lax.axis_index("tp")
    p = tok.shape[0]
    dd = dtok.shape[0]
    own = lx.shape[1]
    extra = x.shape[0]
    rows = qx.shape[1]
    cache = pc_h.shape[1]
    slots = dc_h.shape[2]
    heads = ku.shape[0]
    kl = ku.shape[2]
    key_width = kbuf.shape[0]
    part_q = qd.shape[0]
    part_l = ld.shape[1]
    ql = qu.shape[0]
    chunks = len(outs)
    chunk = outs[0].shape[2]

    pairs = [
        (pt_h, tok),
        (dt_h, dtok),
        (ig_h, ig),
        (qd_h, qd),
        (ld_h, ld),
        (rd_h, rd),
        (pf_h, pfill),
        (df_h, dfill),
        (qg_h, qg),
        (lg_h, lg),
        (qu_h, qu),
        (ru_h, ru),
        (ku_h, ku),
        (pc_h, kbuf),
        (vu_h, vu),
        (dc_h, dbuf),
        (op_h, op),
    ]
    loads = [pltpu.make_async_copy(s, d, in_sem.at[i]) for i, (s, d) in enumerate(pairs)]
    for load in loads:
        load.start()
    early, late, last = loads[:6], loads[6:-1], loads[-1]

    barrier = pltpu.get_barrier_semaphore()

    def greet(dk, dt):
        pl.semaphore_signal(
            barrier,
            inc=1,
            device_id=(lax.rem(me + dk, n), lax.rem(mt + dt, m)),
            device_id_type=MESH,
        )

    for dt in range(m):
        each(0 if dt else 1, n, lambda dk, dt=dt: greet(dk, dt))

    x[...] = jnp.zeros_like(x)
    for load in early:
        load.wait()
    x[0:p, :] = tok[...].astype(F32)
    x[p : p + dd, :] = dtok[...].astype(F32)
    xs = x[...]
    normed = (
        xs * lax.rsqrt(jnp.mean(xs * xs, axis=-1, keepdims=True) + RMS_EPS) * ig[...]
    ).astype(BF16)
    columns = dot_t(normed, qd[...])[0:own]
    qall[mt, 0] = columns[0:p].astype(BF16)
    lx[mt] = jnp.concatenate([dot(normed, ld[...])[0:own], columns], axis=1).astype(BF16)
    raw = dot_t(normed, rd[...])[0:own].astype(BF16).astype(F32)

    pl.semaphore_wait(barrier, n * m - 1)

    def query_copy(dk, dt):
        return pltpu.make_async_remote_copy(
            src_ref=qall.at[mt, 0],
            dst_ref=qall.at[mt, dk],
            send_sem=q_sem.at[0, dt, dk],
            recv_sem=q_sem.at[1, dt, dk],
            device_id=(lax.rem(me + dk, n), lax.rem(mt + dt, m)),
            device_id_type=MESH,
        )

    for dt in range(m):
        each(1, n, lambda dk, dt=dt: query_copy(dk, dt).start())
    l_copies = []
    for dt in range(1, m):
        copy = pltpu.make_async_remote_copy(
            src_ref=lx.at[mt],
            dst_ref=lx.at[mt],
            send_sem=l_sem.at[0, dt],
            recv_sem=l_sem.at[1, dt],
            device_id=(me, lax.rem(mt + dt, m)),
            device_id_type=MESH,
        )
        copy.start()
        l_copies.append(copy)

    for load in late:
        load.wait()
    fill = pfill[...]
    row = lax.broadcasted_iota(jnp.int32, (rows, 1), 0)
    slot = jnp.zeros((rows, 1), jnp.int32)
    for d in range(1, n):
        slot = jnp.where(row >= own + (d - 1) * p, d, slot)
    source = me - slot
    source = jnp.where(source < 0, source + n, source)
    inside = jnp.where(slot == 0, row, row - own - (slot - 1) * p)
    places = fill + source * p + inside
    for b in range(dd):
        places = jnp.where(row == p + b, dfill[b : b + 1, :], places)
    half = ROPE // 2
    turned_axis = heads * ROPE
    lane = lax.broadcasted_iota(jnp.int32, (1, turned_axis), 1)
    frequency = jnp.zeros((1, turned_axis), F32)
    for i in range(half):
        frequency = jnp.where(lane % half == i, THETA ** (-i / half), frequency)
    angles = places.astype(F32) * frequency
    cosine = jnp.cos(angles)
    sine = jnp.sin(angles)
    cos_own = cosine[0:own, 0:half]
    sin_own = sine[0:own, 0:half]
    first, second = raw[:, 0:half], raw[:, half:ROPE]
    new_rope = jnp.concatenate(
        [first * cos_own - second * sin_own, first * sin_own + second * cos_own], axis=1
    )
    gains = qg[...].reshape(1, ql)
    qx[...] = jnp.zeros_like(qx)

    for copy in l_copies:
        copy.wait_recv()
    latent = jnp.concatenate([lx[s, :, 0:part_l].astype(F32) for s in range(m)], axis=1)
    latent = (
        latent * lax.rsqrt(jnp.mean(latent * latent, axis=-1, keepdims=True) + RMS_EPS) * lg[...]
    )
    new_rows = jnp.concatenate([latent, new_rope], axis=1)
    pr_ref[...] = new_rows[0:p].astype(BF16)
    dr_ref[...] = new_rows[p : p + dd].astype(BF16)
    new_bf = jnp.concatenate([new_rows, jnp.zeros((extra - own, key_width), F32)], axis=0)
    new_bf = new_bf.astype(BF16)
    new_latent, new_key = new_bf[:, 0:kl], new_bf[:, kl:key_width]
    for s in range(m):
        qx[s, 0:own, :] = lx[s, :, part_l:].astype(F32)

    for dt in range(m):
        each(1, n, lambda dk, dt=dt: query_copy(dk, dt).wait_recv())
    for d in range(1, n):
        start = own + (d - 1) * p
        qx[:, start : start + p, :] = qall[:, d].astype(F32)
    parts = [qx[s] for s in range(m)]
    square = sum(jnp.sum(v * v, axis=-1, keepdims=True) for v in parts)
    scale = lax.rsqrt(square / ql + RMS_EPS)
    nope = jnp.zeros((rows, qu.shape[1]), F32)
    turn = jnp.zeros((rows, ru.shape[1]), F32)
    for s in range(m):
        lat = (parts[s] * scale * gains[:, s * part_q : (s + 1) * part_q]).astype(BF16)
        nope += dot(lat, qu[s * part_q : (s + 1) * part_q, :])
        turn += dot(lat, ru[s * part_q : (s + 1) * part_q, :])
    nope = nope.astype(BF16)
    turn = turn.astype(BF16).astype(F32)
    above = pltpu.roll(turn, turned_axis - half, 1)
    below = pltpu.roll(turn, half, 1)
    turned = turn * cosine + jnp.where(lane % ROPE < half, -above, below) * sine
    nd = qu.shape[1] // heads
    absorbed = [dot(nope[:, h * nd : (h + 1) * nd], ku[h]) for h in range(heads)]
    turned = [turned[:, h * ROPE : (h + 1) * ROPE] for h in range(heads)]

    score_scale = (NOPE + ROPE) ** (-0.5)
    aq = jnp.concatenate(absorbed, axis=0).astype(BF16)
    tq = jnp.concatenate(turned, axis=0).astype(BF16)
    scores = (
        jnp.concatenate(
            [
                dot(aq, kbuf[0:kl]) + dot(tq, kbuf[kl:key_width]),
                dot_t(aq, new_latent) + dot_t(tq, new_key),
            ],
            axis=1,
        )
        * score_scale
    )
    key = lax.broadcasted_iota(jnp.int32, (1, cache + extra), 1)
    query_place = jnp.concatenate([places] * heads, axis=0)
    fresh = key - cache
    never = jnp.int32(2**30)
    stored = jnp.where(me * cache + key < fill, me * cache + key, never)
    key_place = jnp.where(fresh < 0, stored, jnp.where(fresh < p, fill + me * p + fresh, never))
    allowed = key_place <= query_place
    scores = jnp.where(allowed, scores, NEG_FILL)
    peak = jnp.max(scores, axis=-1, keepdims=True)
    weights = jnp.where(allowed, jnp.exp(scores - peak), 0.0)
    total = jnp.sum(weights, axis=-1, keepdims=True)
    weights = weights.astype(BF16)
    mixed = dot_t(weights[:, 0:cache], kbuf[0:kl]) + dot(weights[:, cache:], new_latent)
    vd = vu.shape[1]
    peak_high = peak.astype(BF16).astype(F32)
    peak_mid = (peak - peak_high).astype(BF16).astype(F32)
    peak_low = peak - peak_high - peak_mid
    total_high = total.astype(BF16).astype(F32)
    total_low = total - total_high
    stat_lane = lax.broadcasted_iota(jnp.int32, (1, csend.shape[2] - vd), 1)
    stats = jnp.where(stat_lane == 0, peak_high, total_low)
    stats = jnp.where(stat_lane == 1, peak_mid, stats)
    stats = jnp.where(stat_lane == 2, peak_low, stats)
    stats = jnp.where(stat_lane == 3, total_high, stats)
    for h in range(heads):
        cut = slice(h * rows, (h + 1) * rows)
        message = jnp.concatenate([dot_t(mixed[cut].astype(BF16), vu[h]), stats[cut]], axis=1)
        stage[0, h * p : (h + 1) * p, :] = message[0:p]
        for d in range(1, n):
            start = own + (d - 1) * p
            stage[d, h * p : (h + 1) * p, :] = message[start : start + p]
    csend[...] = stage[...].astype(BF16)

    def value_copy(d):
        return pltpu.make_async_remote_copy(
            src_ref=csend.at[d],
            dst_ref=crecv.at[d],
            send_sem=c_sem.at[0, d],
            recv_sem=c_sem.at[1, d],
            device_id=(lax.rem(me + n - d, n), mt),
            device_id_type=MESH,
        )

    each(1, n, lambda d: value_copy(d).start())

    dvalues = []
    for b in range(dd):
        at = slice(p + b, p + b + 1)
        qa = jnp.concatenate([v[at] for v in absorbed], axis=0).astype(BF16)
        qt = jnp.concatenate([v[at] for v in turned], axis=0).astype(BF16)
        ds = (
            jnp.concatenate(
                [
                    dot(qa, dbuf[b, 0:kl]) + dot(qt, dbuf[b, kl:key_width]),
                    dot_t(qa, new_latent) + dot_t(qt, new_key),
                ],
                axis=1,
            )
            * score_scale
        )
        dk = lax.broadcasted_iota(jnp.int32, ds.shape, 1)
        ok = (dk < jnp.minimum(dfill[b : b + 1, :], slots)) | (dk == slots + p + b)
        ds = jnp.where(ok, ds, NEG_FILL)
        dpeak = jnp.max(ds, axis=-1, keepdims=True)
        dw = jnp.where(ok, jnp.exp(ds - dpeak), 0.0)
        dtotal = jnp.sum(dw, axis=-1, keepdims=True)
        dw = dw.astype(BF16)
        dmix = (dot_t(dw[:, 0:slots], dbuf[b, 0:kl]) + dot(dw[:, slots:], new_latent)).astype(BF16)
        dvals = [dot_t(dmix, vu[h])[h : h + 1] / dtotal[h : h + 1] for h in range(heads)]
        dvalues.append(jnp.concatenate(dvals, axis=1))
    last.wait()

    def row_copy(buf, sem, dt):
        return pltpu.make_async_remote_copy(
            src_ref=buf.at[mt],
            dst_ref=buf.at[mt],
            send_sem=sem.at[0, dt],
            recv_sem=sem.at[1, dt],
            device_id=(me, lax.rem(mt + dt, m)),
            device_id_type=MESH,
        )

    dbuf_out[mt] = dot(jnp.concatenate(dvalues, axis=0).astype(BF16), op[...]).astype(BF16)
    o_copies = [row_copy(dbuf_out, d_sem, dt) for dt in range(1, m)]
    for copy in o_copies:
        copy.start()

    each(1, n, lambda d: value_copy(d).wait_recv())
    blocks = [csend[0].astype(F32)] + [crecv[d].astype(F32) for d in range(1, n)]

    def peak_of(block):
        return block[:, vd : vd + 1] + block[:, vd + 1 : vd + 2] + block[:, vd + 2 : vd + 3]

    peaks = [peak_of(block) for block in blocks]
    top = functools.reduce(jnp.maximum, peaks)
    merged = jnp.zeros(blocks[0].shape, F32)
    for block, block_peak in zip(blocks, peaks):
        merged += block * jnp.exp(block_peak - top)
    value = merged[:, 0:vd] / (merged[:, vd + 3 : vd + 4] + merged[:, vd + 4 : vd + 5])
    values = jnp.concatenate([value[h * p : (h + 1) * p] for h in range(heads)], axis=1)
    values = values.astype(BF16)
    for c in range(chunks):
        obuf = outs[c]
        obuf[mt] = dot(values, op[:, c * chunk : (c + 1) * chunk]).astype(BF16)
        for dt in range(1, m):
            copy = row_copy(obuf, o_sem.at[c], dt)
            copy.start()
            o_copies.append(copy)
    for copy in o_copies:
        copy.wait_recv()
    do_ref[...] = sum(dbuf_out[s].astype(F32) for s in range(m)).astype(BF16)
    for c in range(chunks):
        out = sum(outs[c][s].astype(F32) for s in range(m))
        po_ref[:, c * chunk : (c + 1) * chunk] = out.astype(BF16)
    for dt in range(m):
        each(1, n, lambda dk, dt=dt: query_copy(dk, dt).wait_send())
    each(1, n, lambda d: value_copy(d).wait_send())
    for copy in l_copies + o_copies:
        copy.wait_send()


def local(n, m, *args):
    (pt, dt, pfill, dfill, pc, dc, ig, qg, lg, qd, ld, rd, qu, ru, ku, vu, op) = args
    p, width = pt.shape
    dd = dt.shape[0]
    own = round_up(p + dd, 8)
    rows = round_up(own + (n - 1) * p, 8)
    extra = round_up(own, 16)
    heads, nd, kl = ku.shape
    chunks = 2
    any_spec = pl.BlockSpec(memory_space=pltpu.HBM)
    vmem = pl.BlockSpec(memory_space=pltpu.VMEM)
    ig, lg = ig[None], lg[None]
    pfill, dfill = pfill[None], dfill[:, None]
    pc, qd, rd = pc.T, qd.T, rd.T
    dc, vu = jnp.swapaxes(dc, 1, 2), jnp.swapaxes(vu, 1, 2)
    like = lambda a: pltpu.VMEM(a.shape, a.dtype)
    scratch = [
        *[like(a) for a in (pt, dt, pfill, dfill, pc, dc, ig, qg, lg)],
        *[like(a) for a in (qd, ld, rd, qu, ru, ku, vu, op)],
        pltpu.VMEM((extra, width), F32),
        pltpu.VMEM((m, n, p, qd.shape[0]), BF16),
        pltpu.VMEM((m, own, ld.shape[1] + qd.shape[0]), BF16),
        pltpu.VMEM((m, rows, qd.shape[0]), F32),
        pltpu.VMEM((n, heads * p, 128), F32),
        pltpu.VMEM((n, heads * p, 128), BF16),
        pltpu.VMEM((n, heads * p, 128), BF16),
        pltpu.VMEM((m, dd, width), BF16),
        [pltpu.VMEM((m, p, width // chunks), BF16)] * chunks,
        pltpu.SemaphoreType.DMA((17,)),
        pltpu.SemaphoreType.DMA((2, m, n)),
        pltpu.SemaphoreType.DMA((2, m)),
        pltpu.SemaphoreType.DMA((2, n)),
        pltpu.SemaphoreType.DMA((2, m)),
        pltpu.SemaphoreType.DMA((chunks, 2, m)),
    ]
    return pl.pallas_call(
        functools.partial(kernel, n, m),
        out_shape=(
            jax.ShapeDtypeStruct((p, width), BF16),
            jax.ShapeDtypeStruct((dd, width), BF16),
            jax.ShapeDtypeStruct((p, pc.shape[0]), BF16),
            jax.ShapeDtypeStruct((dd, pc.shape[0]), BF16),
        ),
        in_specs=[any_spec] * 17,
        out_specs=(vmem,) * 4,
        scratch_shapes=scratch,
        compiler_params=pltpu.CompilerParams(
            collective_id=0, has_side_effects=True, vmem_limit_bytes=60 * 1024 * 1024
        ),
    )(pt, dt, pfill, dfill, pc, dc, ig, qg, lg, qd, ld, rd, qu, ru, ku, vu, op)


def solution(mesh):
    placed = (
        P("kv", None),
        P("kv", None),
        P(),
        P("kv"),
        P("kv", None),
        P("kv", None, None),
        P(),
        P(),
        P(),
        P(None, "tp"),
        P(None, "tp"),
        P(),
        P(None, "tp"),
        P(None, "tp"),
        P("tp", None, None),
        P("tp", None, None),
        P("tp", None),
    )
    return jax.shard_map(
        functools.partial(local, mesh.shape["kv"], mesh.shape["tp"]),
        mesh=mesh,
        in_specs=placed,
        out_specs=(P("kv", None), P("kv", None), P("kv", None), P("kv", None)),
        check_vma=False,
    )
```

```python
import functools
import math

import jax
import jax.numpy as jnp
from jax import lax
from jax.experimental import pallas as pl
from jax.experimental.pallas import tpu as pltpu
from jax.sharding import PartitionSpec as P

NOPE = 64
ROPE = 32
NEG_FILL = -1e30
RMS_EPS = 1e-06
THETA = 10000.0
F32 = jnp.float32
BF16 = jnp.bfloat16
MESH = pl.DeviceIdType.MESH


def dot(a, b):
    return jnp.dot(a, b, preferred_element_type=F32)


def dot_t(a, b):
    return lax.dot_general(a, b, (((1,), (1,)), ((), ())), preferred_element_type=F32)


def each(low, high, body):
    if high - low <= 8:
        for i in range(low, high):
            body(i)
    else:
        lax.fori_loop(low, high, lambda i, carry: (body(i), carry)[1], 0)


def round_up(value, step):
    return -(-value // step) * step


def kernel(
    n,
    m,
    pt_h,
    dt_h,
    pf_h,
    df_h,
    pc_h,
    dc_h,
    ig_h,
    qg_h,
    lg_h,
    qd_h,
    ld_h,
    rd_h,
    qu_h,
    ru_h,
    ku_h,
    vu_h,
    op_h,
    po_ref,
    do_ref,
    pr_ref,
    dr_ref,
    tok,
    dtok,
    pfill,
    dfill,
    kbuf,
    dbuf,
    ig,
    qg,
    lg,
    qd,
    ld,
    rd,
    qu,
    ru,
    ku,
    vu,
    op,
    x,
    qall,
    lx,
    qx,
    stage,
    csend,
    crecv,
    dbuf_out,
    outs,
    in_sem,
    q_sem,
    l_sem,
    c_sem,
    d_sem,
    o_sem,
):
    me = lax.axis_index("kv")
    mt = lax.axis_index("tp")
    p = tok.shape[0]
    dd = dtok.shape[0]
    own = lx.shape[1]
    extra = x.shape[0]
    rows = qx.shape[1]
    cache = pc_h.shape[1]
    slots = dc_h.shape[2]
    heads = ku.shape[0]
    kl = ku.shape[2]
    key_width = kbuf.shape[0]
    part_q = qd.shape[0]
    part_l = ld.shape[1]
    ql = qu.shape[0]
    chunks = len(outs)
    chunk = outs[0].shape[2]

    pairs = [
        (pt_h, tok),
        (dt_h, dtok),
        (ig_h, ig),
        (qd_h, qd),
        (ld_h, ld),
        (rd_h, rd),
        (pf_h, pfill),
        (df_h, dfill),
        (qg_h, qg),
        (lg_h, lg),
        (qu_h, qu),
        (ru_h, ru),
        (ku_h, ku),
        (pc_h, kbuf),
        (vu_h, vu),
        (dc_h, dbuf),
        (op_h, op),
    ]
    loads = [pltpu.make_async_copy(s, d, in_sem.at[i]) for i, (s, d) in enumerate(pairs)]
    for load in loads:
        load.start()
    early, late, last = loads[:6], loads[6:-1], loads[-1]

    barrier = pltpu.get_barrier_semaphore()

    def greet(dk, dt):
        pl.semaphore_signal(
            barrier,
            inc=1,
            device_id=(lax.rem(me + dk, n), lax.rem(mt + dt, m)),
            device_id_type=MESH,
        )

    for dt in range(m):
        each(0 if dt else 1, n, lambda dk, dt=dt: greet(dk, dt))

    x[...] = jnp.zeros_like(x)
    for load in early:
        load.wait()
    x[0:p, :] = tok[...].astype(F32)
    x[p : p + dd, :] = dtok[...].astype(F32)
    xs = x[...]
    normed = (
        xs * lax.rsqrt(jnp.mean(xs * xs, axis=-1, keepdims=True) + RMS_EPS) * ig[...]
    ).astype(BF16)
    columns = dot_t(normed, qd[...])[0:own]
    qall[mt, 0] = columns[0:p].astype(BF16)
    lx[mt] = jnp.concatenate([dot(normed, ld[...])[0:own], columns], axis=1).astype(BF16)
    raw = dot_t(normed, rd[...])[0:own].astype(BF16).astype(F32)

    pl.semaphore_wait(barrier, n * m - 1)

    def query_copy(dk, dt):
        return pltpu.make_async_remote_copy(
            src_ref=qall.at[mt, 0],
            dst_ref=qall.at[mt, dk],
            send_sem=q_sem.at[0, dt, dk],
            recv_sem=q_sem.at[1, dt, dk],
            device_id=(lax.rem(me + dk, n), lax.rem(mt + dt, m)),
            device_id_type=MESH,
        )

    for dt in range(m):
        each(1, n, lambda dk, dt=dt: query_copy(dk, dt).start())
    l_copies = []
    for dt in range(1, m):
        copy = pltpu.make_async_remote_copy(
            src_ref=lx.at[mt],
            dst_ref=lx.at[mt],
            send_sem=l_sem.at[0, dt],
            recv_sem=l_sem.at[1, dt],
            device_id=(me, lax.rem(mt + dt, m)),
            device_id_type=MESH,
        )
        copy.start()
        l_copies.append(copy)

    for load in late:
        load.wait()
    fill = pfill[...]
    row = lax.broadcasted_iota(jnp.int32, (rows, 1), 0)
    slot = jnp.zeros((rows, 1), jnp.int32)
    for d in range(1, n):
        slot = jnp.where(row >= own + (d - 1) * p, d, slot)
    source = me - slot
    source = jnp.where(source < 0, source + n, source)
    inside = jnp.where(slot == 0, row, row - own - (slot - 1) * p)
    places = fill + source * p + inside
    for b in range(dd):
        places = jnp.where(row == p + b, dfill[b : b + 1, :], places)
    half = ROPE // 2
    turned_axis = heads * ROPE
    lane = lax.broadcasted_iota(jnp.int32, (1, turned_axis), 1)
    frequency = jnp.zeros((1, turned_axis), F32)
    for i in range(half):
        frequency = jnp.where(lane % half == i, THETA ** (-i / half), frequency)
    angles = places.astype(F32) * frequency
    cosine = jnp.cos(angles)
    sine = jnp.sin(angles)
    cos_own = cosine[0:own, 0:half]
    sin_own = sine[0:own, 0:half]
    first, second = raw[:, 0:half], raw[:, half:ROPE]
    new_rope = jnp.concatenate(
        [first * cos_own - second * sin_own, first * sin_own + second * cos_own], axis=1
    )
    gains = qg[...].reshape(1, ql)
    qx[...] = jnp.zeros_like(qx)

    for copy in l_copies:
        copy.wait_recv()
    latent = jnp.concatenate([lx[s, :, 0:part_l].astype(F32) for s in range(m)], axis=1)
    latent = (
        latent * lax.rsqrt(jnp.mean(latent * latent, axis=-1, keepdims=True) + RMS_EPS) * lg[...]
    )
    new_rows = jnp.concatenate([latent, new_rope], axis=1)
    pr_ref[...] = new_rows[0:p].astype(BF16)
    dr_ref[...] = new_rows[p : p + dd].astype(BF16)
    new_bf = jnp.concatenate([new_rows, jnp.zeros((extra - own, key_width), F32)], axis=0)
    new_bf = new_bf.astype(BF16)
    new_latent, new_key = new_bf[:, 0:kl], new_bf[:, kl:key_width]
    for s in range(m):
        qx[s, 0:own, :] = lx[s, :, part_l:].astype(F32)

    for dt in range(m):
        each(1, n, lambda dk, dt=dt: query_copy(dk, dt).wait_recv())
    for d in range(1, n):
        start = own + (d - 1) * p
        qx[:, start : start + p, :] = qall[:, d].astype(F32)
    parts = [qx[s] for s in range(m)]
    square = sum(jnp.sum(v * v, axis=-1, keepdims=True) for v in parts)
    scale = lax.rsqrt(square / ql + RMS_EPS)
    nope = jnp.zeros((rows, qu.shape[1]), F32)
    turn = jnp.zeros((rows, ru.shape[1]), F32)
    for s in range(m):
        lat = (parts[s] * scale * gains[:, s * part_q : (s + 1) * part_q]).astype(BF16)
        nope += dot(lat, qu[s * part_q : (s + 1) * part_q, :])
        turn += dot(lat, ru[s * part_q : (s + 1) * part_q, :])
    nope = nope.astype(BF16)
    turn = turn.astype(BF16).astype(F32)
    above = pltpu.roll(turn, turned_axis - half, 1)
    below = pltpu.roll(turn, half, 1)
    turned = turn * cosine + jnp.where(lane % ROPE < half, -above, below) * sine
    nd = qu.shape[1] // heads
    absorbed = [dot(nope[:, h * nd : (h + 1) * nd], ku[h]) for h in range(heads)]
    turned = [turned[:, h * ROPE : (h + 1) * ROPE] for h in range(heads)]

    score_scale = (NOPE + ROPE) ** (-0.5)
    aq = jnp.concatenate(absorbed, axis=0).astype(BF16)
    tq = jnp.concatenate(turned, axis=0).astype(BF16)
    scores = (
        jnp.concatenate(
            [
                dot(aq, kbuf[0:kl]) + dot(tq, kbuf[kl:key_width]),
                dot_t(aq, new_latent) + dot_t(tq, new_key),
            ],
            axis=1,
        )
        * score_scale
    )
    key = lax.broadcasted_iota(jnp.int32, (1, cache + extra), 1)
    query_place = jnp.concatenate([places] * heads, axis=0)
    fresh = key - cache
    never = jnp.int32(2**30)
    stored = jnp.where(me * cache + key < fill, me * cache + key, never)
    key_place = jnp.where(fresh < 0, stored, jnp.where(fresh < p, fill + me * p + fresh, never))
    allowed = key_place <= query_place
    scores = jnp.where(allowed, scores, NEG_FILL)
    peak = jnp.max(scores, axis=-1, keepdims=True)
    weights = jnp.where(allowed, jnp.exp(scores - peak), 0.0)
    total = jnp.sum(weights, axis=-1, keepdims=True)
    weights = weights.astype(BF16)
    mixed = dot_t(weights[:, 0:cache], kbuf[0:kl]) + dot(weights[:, cache:], new_latent)
    vd = vu.shape[1]
    peak_high = peak.astype(BF16).astype(F32)
    peak_mid = (peak - peak_high).astype(BF16).astype(F32)
    peak_low = peak - peak_high - peak_mid
    total_high = total.astype(BF16).astype(F32)
    total_low = total - total_high
    stat_lane = lax.broadcasted_iota(jnp.int32, (1, csend.shape[2] - vd), 1)
    stats = jnp.where(stat_lane == 0, peak_high, total_low)
    stats = jnp.where(stat_lane == 1, peak_mid, stats)
    stats = jnp.where(stat_lane == 2, peak_low, stats)
    stats = jnp.where(stat_lane == 3, total_high, stats)
    for h in range(heads):
        cut = slice(h * rows, (h + 1) * rows)
        message = jnp.concatenate([dot_t(mixed[cut].astype(BF16), vu[h]), stats[cut]], axis=1)
        stage[0, h * p : (h + 1) * p, :] = message[0:p]
        for d in range(1, n):
            start = own + (d - 1) * p
            stage[d, h * p : (h + 1) * p, :] = message[start : start + p]
    csend[...] = stage[...].astype(BF16)

    def value_copy(d):
        return pltpu.make_async_remote_copy(
            src_ref=csend.at[d],
            dst_ref=crecv.at[d],
            send_sem=c_sem.at[0, d],
            recv_sem=c_sem.at[1, d],
            device_id=(lax.rem(me + n - d, n), mt),
            device_id_type=MESH,
        )

    each(1, n, lambda d: value_copy(d).start())

    dvalues = []
    for b in range(dd):
        at = slice(p + b, p + b + 1)
        qa = jnp.concatenate([v[at] for v in absorbed], axis=0).astype(BF16)
        qt = jnp.concatenate([v[at] for v in turned], axis=0).astype(BF16)
        ds = (
            jnp.concatenate(
                [
                    dot(qa, dbuf[b, 0:kl]) + dot(qt, dbuf[b, kl:key_width]),
                    dot_t(qa, new_latent) + dot_t(qt, new_key),
                ],
                axis=1,
            )
            * score_scale
        )
        dk = lax.broadcasted_iota(jnp.int32, ds.shape, 1)
        ok = (dk < jnp.minimum(dfill[b : b + 1, :], slots)) | (dk == slots + p + b)
        ds = jnp.where(ok, ds, NEG_FILL)
        dpeak = jnp.max(ds, axis=-1, keepdims=True)
        dw = jnp.where(ok, jnp.exp(ds - dpeak), 0.0)
        dtotal = jnp.sum(dw, axis=-1, keepdims=True)
        dw = dw.astype(BF16)
        dmix = (dot_t(dw[:, 0:slots], dbuf[b, 0:kl]) + dot(dw[:, slots:], new_latent)).astype(BF16)
        dvals = [dot_t(dmix, vu[h])[h : h + 1] / dtotal[h : h + 1] for h in range(heads)]
        dvalues.append(jnp.concatenate(dvals, axis=1))
    last.wait()

    def row_copy(buf, sem, dt):
        return pltpu.make_async_remote_copy(
            src_ref=buf.at[mt],
            dst_ref=buf.at[mt],
            send_sem=sem.at[0, dt],
            recv_sem=sem.at[1, dt],
            device_id=(me, lax.rem(mt + dt, m)),
            device_id_type=MESH,
        )

    dbuf_out[mt] = dot(jnp.concatenate(dvalues, axis=0).astype(BF16), op[...]).astype(BF16)
    o_copies = [row_copy(dbuf_out, d_sem, dt) for dt in range(1, m)]
    for copy in o_copies:
        copy.start()

    each(1, n, lambda d: value_copy(d).wait_recv())
    blocks = [csend[0].astype(F32)] + [crecv[d].astype(F32) for d in range(1, n)]

    def peak_of(block):
        return block[:, vd : vd + 1] + block[:, vd + 1 : vd + 2] + block[:, vd + 2 : vd + 3]

    peaks = [peak_of(block) for block in blocks]
    top = functools.reduce(jnp.maximum, peaks)
    merged = jnp.zeros(blocks[0].shape, F32)
    for block, block_peak in zip(blocks, peaks):
        merged += block * jnp.exp(block_peak - top)
    value = merged[:, 0:vd] / (merged[:, vd + 3 : vd + 4] + merged[:, vd + 4 : vd + 5])
    values = jnp.concatenate([value[h * p : (h + 1) * p] for h in range(heads)], axis=1)
    values = values.astype(BF16)
    for c in range(chunks):
        obuf = outs[c]
        obuf[mt] = dot(values, op[:, c * chunk : (c + 1) * chunk]).astype(BF16)
        for dt in range(1, m):
            copy = row_copy(obuf, o_sem.at[c], dt)
            copy.start()
            o_copies.append(copy)
    for copy in o_copies:
        copy.wait_recv()
    do_ref[...] = sum(dbuf_out[s].astype(F32) for s in range(m)).astype(BF16)
    for c in range(chunks):
        out = sum(outs[c][s].astype(F32) for s in range(m))
        po_ref[:, c * chunk : (c + 1) * chunk] = out.astype(BF16)
    for dt in range(m):
        each(1, n, lambda dk, dt=dt: query_copy(dk, dt).wait_send())
    each(1, n, lambda d: value_copy(d).wait_send())
    for copy in l_copies + o_copies:
        copy.wait_send()


def put_out(*refs):
    count = len(refs) // 2
    sem = refs[-1]
    copies = [
        pltpu.make_async_copy(refs[i], refs[count + i], sem.at[i]) for i in range(count)
    ]
    for copy in copies:
        copy.start()
    for copy in copies:
        copy.wait()


def local(n, m, *args):
    (pt, dt, pfill, dfill, pc, dc, ig, qg, lg, qd, ld, rd, qu, ru, ku, vu, op) = args
    p, width = pt.shape
    dd = dt.shape[0]
    own = round_up(p + dd, 8)
    rows = round_up(own + (n - 1) * p, 8)
    extra = round_up(own, 16)
    heads, nd, kl = ku.shape
    chunks = 2
    any_spec = pl.BlockSpec(memory_space=pltpu.HBM)
    vmem = pl.BlockSpec(memory_space=pltpu.VMEM)
    ig, lg = ig[None], lg[None]
    pfill, dfill = pfill[None], dfill[:, None]
    pc, qd, rd = pc.T, qd.T, rd.T
    dc, vu = jnp.swapaxes(dc, 1, 2), jnp.swapaxes(vu, 1, 2)
    like = lambda a: pltpu.VMEM(a.shape, a.dtype)
    scratch = [
        *[like(a) for a in (pt, dt, pfill, dfill, pc, dc, ig, qg, lg)],
        *[like(a) for a in (qd, ld, rd, qu, ru, ku, vu, op)],
        pltpu.VMEM((extra, width), F32),
        pltpu.VMEM((m, n, p, qd.shape[0]), BF16),
        pltpu.VMEM((m, own, ld.shape[1] + qd.shape[0]), BF16),
        pltpu.VMEM((m, rows, qd.shape[0]), F32),
        pltpu.VMEM((n, heads * p, 128), F32),
        pltpu.VMEM((n, heads * p, 128), BF16),
        pltpu.VMEM((n, heads * p, 128), BF16),
        pltpu.VMEM((m, dd, width), BF16),
        [pltpu.VMEM((m, p, width // chunks), BF16)] * chunks,
        pltpu.SemaphoreType.DMA((17,)),
        pltpu.SemaphoreType.DMA((2, m, n)),
        pltpu.SemaphoreType.DMA((2, m)),
        pltpu.SemaphoreType.DMA((2, n)),
        pltpu.SemaphoreType.DMA((2, m)),
        pltpu.SemaphoreType.DMA((chunks, 2, m)),
    ]
    held = pl.pallas_call(
        functools.partial(kernel, n, m),
        out_shape=(
            pltpu.VMEM((p, width), BF16),
            pltpu.VMEM((dd, width), BF16),
            pltpu.VMEM((p, pc.shape[0]), BF16),
            pltpu.VMEM((dd, pc.shape[0]), BF16),
        ),
        in_specs=[any_spec] * 17,
        out_specs=(vmem,) * 4,
        scratch_shapes=scratch,
        compiler_params=pltpu.CompilerParams(
            collective_id=0, has_side_effects=True, vmem_limit_bytes=60 * 1024 * 1024
        ),
    )(pt, dt, pfill, dfill, pc, dc, ig, qg, lg, qd, ld, rd, qu, ru, ku, vu, op)
    return pl.pallas_call(
        put_out,
        out_shape=tuple(jax.ShapeDtypeStruct(a.shape, a.dtype) for a in held),
        in_specs=[vmem] * len(held),
        out_specs=(any_spec,) * len(held),
        scratch_shapes=[pltpu.SemaphoreType.DMA((len(held),))],
        compiler_params=pltpu.CompilerParams(vmem_limit_bytes=1024 * 1024),
    )(*held)


def solution(mesh):
    placed = (
        P("kv", None),
        P("kv", None),
        P(),
        P("kv"),
        P("kv", None),
        P("kv", None, None),
        P(),
        P(),
        P(),
        P(None, "tp"),
        P(None, "tp"),
        P(),
        P(None, "tp"),
        P(None, "tp"),
        P("tp", None, None),
        P("tp", None, None),
        P("tp", None),
    )
    return jax.shard_map(
        functools.partial(local, mesh.shape["kv"], mesh.shape["tp"]),
        mesh=mesh,
        in_specs=placed,
        out_specs=(P("kv", None), P("kv", None), P("kv", None), P("kv", None)),
        check_vma=False,
    )
```

```python
import functools
import math

import jax
import jax.numpy as jnp
from jax import lax
from jax.experimental import pallas as pl
from jax.experimental.pallas import tpu as pltpu
from jax.sharding import PartitionSpec as P

NOPE = 64
ROPE = 32
NEG_FILL = -1e30
RMS_EPS = 1e-06
THETA = 10000.0
F32 = jnp.float32
BF16 = jnp.bfloat16
MESH = pl.DeviceIdType.MESH


def dot(a, b):
    return jnp.dot(a, b, preferred_element_type=F32)


def dot_t(a, b):
    return lax.dot_general(a, b, (((1,), (1,)), ((), ())), preferred_element_type=F32)


def each(low, high, body):
    if high - low <= 8:
        for i in sorted(range(low, high), key=lambda i: -min(i, high - i)):
            body(i)
    else:
        lax.fori_loop(low, high, lambda i, carry: (body(i), carry)[1], 0)


def round_up(value, step):
    return -(-value // step) * step


def kernel(
    n,
    m,
    pt_h,
    dt_h,
    pf_h,
    df_h,
    pc_h,
    dc_h,
    ig_h,
    qg_h,
    lg_h,
    qd_h,
    ld_h,
    rd_h,
    qu_h,
    ru_h,
    ku_h,
    vu_h,
    op_h,
    po_ref,
    do_ref,
    pr_ref,
    dr_ref,
    tok,
    dtok,
    pfill,
    dfill,
    kbuf,
    dbuf,
    ig,
    qg,
    lg,
    qd,
    ld,
    rd,
    qu,
    ru,
    ku,
    vu,
    op,
    x,
    qall,
    lx,
    qx,
    stage,
    csend,
    crecv,
    dbuf_out,
    outs,
    in_sem,
    q_sem,
    l_sem,
    c_sem,
    d_sem,
    o_sem,
):
    me = lax.axis_index("kv")
    mt = lax.axis_index("tp")
    p = tok.shape[0]
    dd = dtok.shape[0]
    own = lx.shape[1]
    extra = x.shape[0]
    rows = qx.shape[1]
    cache = pc_h.shape[1]
    slots = dc_h.shape[2]
    heads = ku.shape[0]
    kl = ku.shape[2]
    key_width = kbuf.shape[0]
    part_q = qd.shape[0]
    part_l = ld.shape[1]
    ql = qu.shape[0]
    chunks = len(outs)
    chunk = outs[0].shape[2]

    pairs = [
        (pt_h, tok),
        (dt_h, dtok),
        (ig_h, ig),
        (qd_h, qd),
        (ld_h, ld),
        (rd_h, rd),
        (pf_h, pfill),
        (df_h, dfill),
        (qg_h, qg),
        (lg_h, lg),
        (qu_h, qu),
        (ru_h, ru),
        (ku_h, ku),
        (pc_h, kbuf),
        (vu_h, vu),
        (dc_h, dbuf),
        (op_h, op),
    ]
    loads = [pltpu.make_async_copy(s, d, in_sem.at[i]) for i, (s, d) in enumerate(pairs)]
    early, late, last = loads[:6], loads[6:-1], loads[-1]
    for load in early:
        load.start()

    barrier = pltpu.get_barrier_semaphore()

    def greet(dk, dt):
        pl.semaphore_signal(
            barrier,
            inc=1,
            device_id=(lax.rem(me + dk, n), lax.rem(mt + dt, m)),
            device_id_type=MESH,
        )

    for dt in range(m):
        each(0 if dt else 1, n, lambda dk, dt=dt: greet(dk, dt))

    x[...] = jnp.zeros_like(x)
    for load in early:
        load.wait()
    for load in loads[6:]:
        load.start()
    x[0:p, :] = tok[...].astype(F32)
    x[p : p + dd, :] = dtok[...].astype(F32)
    xs = x[...]
    normed = (
        xs * lax.rsqrt(jnp.mean(xs * xs, axis=-1, keepdims=True) + RMS_EPS) * ig[...]
    ).astype(BF16)
    columns = dot_t(normed, qd[...])[0:own]
    qall[mt, 0] = columns[0:p].astype(BF16)
    lx[mt] = jnp.concatenate([dot(normed, ld[...])[0:own], columns], axis=1).astype(BF16)
    raw = dot_t(normed, rd[...])[0:own].astype(BF16).astype(F32)

    pl.semaphore_wait(barrier, n * m - 1)

    def query_copy(dk, dt):
        return pltpu.make_async_remote_copy(
            src_ref=qall.at[mt, 0],
            dst_ref=qall.at[mt, dk],
            send_sem=q_sem.at[0, dt, dk],
            recv_sem=q_sem.at[1, dt, dk],
            device_id=(lax.rem(me + dk, n), lax.rem(mt + dt, m)),
            device_id_type=MESH,
        )

    l_copies = []
    for dt in range(1, m):
        copy = pltpu.make_async_remote_copy(
            src_ref=lx.at[mt],
            dst_ref=lx.at[mt],
            send_sem=l_sem.at[0, dt],
            recv_sem=l_sem.at[1, dt],
            device_id=(me, lax.rem(mt + dt, m)),
            device_id_type=MESH,
        )
        copy.start()
        l_copies.append(copy)
    for dt in reversed(range(m)):
        each(1, n, lambda dk, dt=dt: query_copy(dk, dt).start())

    for load in late:
        load.wait()
    fill = pfill[...]
    row = lax.broadcasted_iota(jnp.int32, (rows, 1), 0)
    slot = jnp.zeros((rows, 1), jnp.int32)
    for d in range(1, n):
        slot = jnp.where(row >= own + (d - 1) * p, d, slot)
    source = me - slot
    source = jnp.where(source < 0, source + n, source)
    inside = jnp.where(slot == 0, row, row - own - (slot - 1) * p)
    places = fill + source * p + inside
    for b in range(dd):
        places = jnp.where(row == p + b, dfill[b : b + 1, :], places)
    half = ROPE // 2
    turned_axis = heads * ROPE
    lane = lax.broadcasted_iota(jnp.int32, (1, turned_axis), 1)
    frequency = jnp.zeros((1, turned_axis), F32)
    for i in range(half):
        frequency = jnp.where(lane % half == i, THETA ** (-i / half), frequency)
    angles = places.astype(F32) * frequency
    cosine = jnp.cos(angles)
    sine = jnp.sin(angles)
    cos_own = cosine[0:own, 0:half]
    sin_own = sine[0:own, 0:half]
    first, second = raw[:, 0:half], raw[:, half:ROPE]
    new_rope = jnp.concatenate(
        [first * cos_own - second * sin_own, first * sin_own + second * cos_own], axis=1
    )
    gains = qg[...].reshape(1, ql)
    qx[...] = jnp.zeros_like(qx)

    for copy in l_copies:
        copy.wait_recv()
    latent = jnp.concatenate([lx[s, :, 0:part_l].astype(F32) for s in range(m)], axis=1)
    latent = (
        latent * lax.rsqrt(jnp.mean(latent * latent, axis=-1, keepdims=True) + RMS_EPS) * lg[...]
    )
    new_rows = jnp.concatenate([latent, new_rope], axis=1)
    pr_ref[...] = new_rows[0:p].astype(BF16)
    dr_ref[...] = new_rows[p : p + dd].astype(BF16)
    new_bf = jnp.concatenate([new_rows, jnp.zeros((extra - own, key_width), F32)], axis=0)
    new_bf = new_bf.astype(BF16)
    new_latent, new_key = new_bf[:, 0:kl], new_bf[:, kl:key_width]
    for s in range(m):
        qx[s, 0:own, :] = lx[s, :, part_l:].astype(F32)

    for dt in range(m):
        each(1, n, lambda dk, dt=dt: query_copy(dk, dt).wait_recv())
    for d in range(1, n):
        start = own + (d - 1) * p
        qx[:, start : start + p, :] = qall[:, d].astype(F32)
    parts = [qx[s] for s in range(m)]
    square = sum(jnp.sum(v * v, axis=-1, keepdims=True) for v in parts)
    scale = lax.rsqrt(square / ql + RMS_EPS)
    nope = jnp.zeros((rows, qu.shape[1]), F32)
    turn = jnp.zeros((rows, ru.shape[1]), F32)
    for s in range(m):
        lat = (parts[s] * scale * gains[:, s * part_q : (s + 1) * part_q]).astype(BF16)
        nope += dot(lat, qu[s * part_q : (s + 1) * part_q, :])
        turn += dot(lat, ru[s * part_q : (s + 1) * part_q, :])
    nope = nope.astype(BF16)
    turn = turn.astype(BF16).astype(F32)
    above = pltpu.roll(turn, turned_axis - half, 1)
    below = pltpu.roll(turn, half, 1)
    turned = turn * cosine + jnp.where(lane % ROPE < half, -above, below) * sine
    nd = qu.shape[1] // heads
    absorbed = [dot(nope[:, h * nd : (h + 1) * nd], ku[h]) for h in range(heads)]
    turned = [turned[:, h * ROPE : (h + 1) * ROPE] for h in range(heads)]

    score_scale = (NOPE + ROPE) ** (-0.5)
    aq = jnp.concatenate(absorbed, axis=0).astype(BF16)
    tq = jnp.concatenate(turned, axis=0).astype(BF16)
    scores = (
        jnp.concatenate(
            [
                dot(aq, kbuf[0:kl]) + dot(tq, kbuf[kl:key_width]),
                dot_t(aq, new_latent) + dot_t(tq, new_key),
            ],
            axis=1,
        )
        * score_scale
    )
    key = lax.broadcasted_iota(jnp.int32, (1, cache + extra), 1)
    query_place = jnp.concatenate([places] * heads, axis=0)
    fresh = key - cache
    never = jnp.int32(2**30)
    stored = jnp.where(me * cache + key < fill, me * cache + key, never)
    key_place = jnp.where(fresh < 0, stored, jnp.where(fresh < p, fill + me * p + fresh, never))
    allowed = key_place <= query_place
    scores = jnp.where(allowed, scores, NEG_FILL)
    peak = jnp.max(scores, axis=-1, keepdims=True)
    weights = jnp.where(allowed, jnp.exp(scores - peak), 0.0)
    total = jnp.sum(weights, axis=-1, keepdims=True)
    weights = weights.astype(BF16)
    mixed = dot_t(weights[:, 0:cache], kbuf[0:kl]) + dot(weights[:, cache:], new_latent)
    vd = vu.shape[1]
    peak_high = peak.astype(BF16).astype(F32)
    peak_mid = (peak - peak_high).astype(BF16).astype(F32)
    peak_low = peak - peak_high - peak_mid
    total_high = total.astype(BF16).astype(F32)
    total_low = total - total_high
    stat_lane = lax.broadcasted_iota(jnp.int32, (1, csend.shape[2] - vd), 1)
    stats = jnp.where(stat_lane == 0, peak_high, total_low)
    stats = jnp.where(stat_lane == 1, peak_mid, stats)
    stats = jnp.where(stat_lane == 2, peak_low, stats)
    stats = jnp.where(stat_lane == 3, total_high, stats)
    for h in range(heads):
        cut = slice(h * rows, (h + 1) * rows)
        message = jnp.concatenate([dot_t(mixed[cut].astype(BF16), vu[h]), stats[cut]], axis=1)
        stage[0, h * p : (h + 1) * p, :] = message[0:p]
        for d in range(1, n):
            start = own + (d - 1) * p
            stage[d, h * p : (h + 1) * p, :] = message[start : start + p]
    csend[...] = stage[...].astype(BF16)

    def value_copy(d):
        return pltpu.make_async_remote_copy(
            src_ref=csend.at[d],
            dst_ref=crecv.at[d],
            send_sem=c_sem.at[0, d],
            recv_sem=c_sem.at[1, d],
            device_id=(lax.rem(me + n - d, n), mt),
            device_id_type=MESH,
        )

    each(1, n, lambda d: value_copy(d).start())

    dvalues = []
    for b in range(dd):
        at = slice(p + b, p + b + 1)
        qa = jnp.concatenate([v[at] for v in absorbed], axis=0).astype(BF16)
        qt = jnp.concatenate([v[at] for v in turned], axis=0).astype(BF16)
        ds = (
            jnp.concatenate(
                [
                    dot(qa, dbuf[b, 0:kl]) + dot(qt, dbuf[b, kl:key_width]),
                    dot_t(qa, new_latent) + dot_t(qt, new_key),
                ],
                axis=1,
            )
            * score_scale
        )
        dk = lax.broadcasted_iota(jnp.int32, ds.shape, 1)
        ok = (dk < jnp.minimum(dfill[b : b + 1, :], slots)) | (dk == slots + p + b)
        ds = jnp.where(ok, ds, NEG_FILL)
        dpeak = jnp.max(ds, axis=-1, keepdims=True)
        dw = jnp.where(ok, jnp.exp(ds - dpeak), 0.0)
        dtotal = jnp.sum(dw, axis=-1, keepdims=True)
        dw = dw.astype(BF16)
        dmix = (dot_t(dw[:, 0:slots], dbuf[b, 0:kl]) + dot(dw[:, slots:], new_latent)).astype(BF16)
        dvals = [dot_t(dmix, vu[h])[h : h + 1] / dtotal[h : h + 1] for h in range(heads)]
        dvalues.append(jnp.concatenate(dvals, axis=1))
    last.wait()

    def row_copy(buf, sem, dt):
        return pltpu.make_async_remote_copy(
            src_ref=buf.at[mt],
            dst_ref=buf.at[mt],
            send_sem=sem.at[0, dt],
            recv_sem=sem.at[1, dt],
            device_id=(me, lax.rem(mt + dt, m)),
            device_id_type=MESH,
        )

    dbuf_out[mt] = dot(jnp.concatenate(dvalues, axis=0).astype(BF16), op[...]).astype(BF16)
    o_copies = [row_copy(dbuf_out, d_sem, dt) for dt in range(1, m)]
    for copy in o_copies:
        copy.start()

    each(1, n, lambda d: value_copy(d).wait_recv())
    blocks = [csend[0].astype(F32)] + [crecv[d].astype(F32) for d in range(1, n)]

    def peak_of(block):
        return block[:, vd : vd + 1] + block[:, vd + 1 : vd + 2] + block[:, vd + 2 : vd + 3]

    peaks = [peak_of(block) for block in blocks]
    top = functools.reduce(jnp.maximum, peaks)
    merged = jnp.zeros(blocks[0].shape, F32)
    for block, block_peak in zip(blocks, peaks):
        merged += block * jnp.exp(block_peak - top)
    value = merged[:, 0:vd] / (merged[:, vd + 3 : vd + 4] + merged[:, vd + 4 : vd + 5])
    values = jnp.concatenate([value[h * p : (h + 1) * p] for h in range(heads)], axis=1)
    values = values.astype(BF16)
    for c in range(chunks):
        obuf = outs[c]
        obuf[mt] = dot(values, op[:, c * chunk : (c + 1) * chunk]).astype(BF16)
        for dt in range(1, m):
            copy = row_copy(obuf, o_sem.at[c], dt)
            copy.start()
            o_copies.append(copy)
    for copy in o_copies[: m - 1]:
        copy.wait_recv()
    do_ref[...] = sum(dbuf_out[s].astype(F32) for s in range(m)).astype(BF16)
    for c in range(chunks):
        for copy in o_copies[(c + 1) * (m - 1) : (c + 2) * (m - 1)]:
            copy.wait_recv()
        out = sum(outs[c][s].astype(F32) for s in range(m))
        po_ref[:, c * chunk : (c + 1) * chunk] = out.astype(BF16)
    for dt in range(m):
        each(1, n, lambda dk, dt=dt: query_copy(dk, dt).wait_send())
    each(1, n, lambda d: value_copy(d).wait_send())
    for copy in l_copies + o_copies:
        copy.wait_send()


def put_out(*refs):
    count = len(refs) // 2
    sem = refs[-1]
    copies = [
        pltpu.make_async_copy(refs[i], refs[count + i], sem.at[i]) for i in range(count)
    ]
    for copy in copies:
        copy.start()
    for copy in copies:
        copy.wait()


def local(n, m, *args):
    (pt, dt, pfill, dfill, pc, dc, ig, qg, lg, qd, ld, rd, qu, ru, ku, vu, op) = args
    p, width = pt.shape
    dd = dt.shape[0]
    own = round_up(p + dd, 8)
    rows = round_up(own + (n - 1) * p, 8)
    extra = round_up(own, 16)
    heads, nd, kl = ku.shape
    chunks = 1
    any_spec = pl.BlockSpec(memory_space=pltpu.HBM)
    vmem = pl.BlockSpec(memory_space=pltpu.VMEM)
    ig, lg = ig[None], lg[None]
    pfill, dfill = pfill[None], dfill[:, None]
    pc, qd, rd = pc.T, qd.T, rd.T
    dc, vu = jnp.swapaxes(dc, 1, 2), jnp.swapaxes(vu, 1, 2)
    like = lambda a: pltpu.VMEM(a.shape, a.dtype)
    scratch = [
        *[like(a) for a in (pt, dt, pfill, dfill, pc, dc, ig, qg, lg)],
        *[like(a) for a in (qd, ld, rd, qu, ru, ku, vu, op)],
        pltpu.VMEM((extra, width), F32),
        pltpu.VMEM((m, n, p, qd.shape[0]), BF16),
        pltpu.VMEM((m, own, ld.shape[1] + qd.shape[0]), BF16),
        pltpu.VMEM((m, rows, qd.shape[0]), F32),
        pltpu.VMEM((n, heads * p, 128), F32),
        pltpu.VMEM((n, heads * p, 128), BF16),
        pltpu.VMEM((n, heads * p, 128), BF16),
        pltpu.VMEM((m, dd, width), BF16),
        [pltpu.VMEM((m, p, width // chunks), BF16)] * chunks,
        pltpu.SemaphoreType.DMA((17,)),
        pltpu.SemaphoreType.DMA((2, m, n)),
        pltpu.SemaphoreType.DMA((2, m)),
        pltpu.SemaphoreType.DMA((2, n)),
        pltpu.SemaphoreType.DMA((2, m)),
        pltpu.SemaphoreType.DMA((chunks, 2, m)),
    ]
    held = pl.pallas_call(
        functools.partial(kernel, n, m),
        out_shape=(
            pltpu.VMEM((p, width), BF16),
            pltpu.VMEM((dd, width), BF16),
            pltpu.VMEM((p, pc.shape[0]), BF16),
            pltpu.VMEM((dd, pc.shape[0]), BF16),
        ),
        in_specs=[any_spec] * 17,
        out_specs=(vmem,) * 4,
        scratch_shapes=scratch,
        compiler_params=pltpu.CompilerParams(
            collective_id=0, has_side_effects=True, vmem_limit_bytes=60 * 1024 * 1024
        ),
    )(pt, dt, pfill, dfill, pc, dc, ig, qg, lg, qd, ld, rd, qu, ru, ku, vu, op)
    return pl.pallas_call(
        put_out,
        out_shape=tuple(jax.ShapeDtypeStruct(a.shape, a.dtype) for a in held),
        in_specs=[vmem] * len(held),
        out_specs=(any_spec,) * len(held),
        scratch_shapes=[pltpu.SemaphoreType.DMA((len(held),))],
        compiler_params=pltpu.CompilerParams(vmem_limit_bytes=1024 * 1024),
    )(*held)


def solution(mesh):
    placed = (
        P("kv", None),
        P("kv", None),
        P(),
        P("kv"),
        P("kv", None),
        P("kv", None, None),
        P(),
        P(),
        P(),
        P(None, "tp"),
        P(None, "tp"),
        P(),
        P(None, "tp"),
        P(None, "tp"),
        P("tp", None, None),
        P("tp", None, None),
        P("tp", None),
    )
    return jax.shard_map(
        functools.partial(local, mesh.shape["kv"], mesh.shape["tp"]),
        mesh=mesh,
        in_specs=placed,
        out_specs=(P("kv", None), P("kv", None), P("kv", None), P("kv", None)),
        check_vma=False,
    )
```
